32 devices in a mesh: fs: 16 (over z, y, x), tp: 2 (over core).
Axes of the slice: x: 2, y: 2, z: 4, core: 2. Of those that a mesh axis runs over, the one named last changes fastest.
Arguments:
- inputs: bfloat16 [8192, 2048], P('fs', 'tp'), may hold values from -6 to 6
- value_cotangent: bfloat16 [8192, 2048], P('fs', 'tp'), may hold values from -6 to 6
- first_map: bfloat16 [8192, 2048], P('fs', 'tp'), may hold values from -6 to 6
- second_map: bfloat16 [8192, 2048], P('fs', 'tp'), may hold values from -6 to 6
- lambdas: float32 [16], P('tp'), may hold values from 0.3 to 0.8
- head_gain: float32 [128], replicated, may hold values from 0.1 to 1.9
- output_cotangent: bfloat16 [8192, 2048], P('fs', 'tp'), may hold values from -6 to 6
- value_factor: bfloat16 [2048, 256], replicated, may hold values from -0.125 to 0.125
- output_factor: bfloat16 [2048, 256], replicated, may hold values from -0.125 to 0.125
- value_weight: float32 [2048, 2048], P('fs', 'tp'), may hold values from -0.125 to 0.125
- output_weight: float32 [2048, 2048], P('tp', 'fs'), may hold values from -0.125 to 0.125
- value_moment: float32 [256, 2048], P('fs', 'tp'), may hold values from -6 to 6
- value_second: float32 [256, 2048], P('fs', 'tp'), may hold values from 0.25 to 4
- output_moment: float32 [256, 2048], P('fs', 'tp'), may hold values from -6 to 6
- output_second: float32 [256, 2048], P('fs', 'tp'), may hold values from 0.25 to 4
Outputs:
- value_master: float32 [2048, 2048], P('fs', 'tp')
- output_master: float32 [2048, 2048], P('tp', 'fs')
- value_moment_new: float32 [256, 2048], P('fs', 'tp')
- value_second_new: float32 [256, 2048], P('fs', 'tp')
- output_moment_new: float32 [256, 2048], P('fs', 'tp')
- output_second_new: float32 [256, 2048], P('fs', 'tp')
- value_copy: bfloat16 [2048, 2048], P(None, 'tp')
- output_copy: bfloat16 [2048, 2048], P('tp')
The draws below stay inside these ranges and needn't reach their ends.
All inputs are finite; a program needn't handle non-finite values.
Results may differ from the reference program's by a relative error of at most 0.0027.
Values may be sent and summed in bfloat16 or wider, within the bound.
A program may use at most 64 MiB of HBM per device.

```python
import math
import jax
import jax.numpy as jnp
from jax import lax

D = 2048
H = 16
VD = 128
R = 256
TOKENS = 8192


def block_scale(own_key, extent, pieces, smallest, high):
    loudness, own = 1.0, jax.random.fold_in(own_key, 6)
    for dim, blocks in pieces:
        draws = jnp.exp(jax.random.uniform(jax.random.fold_in(own, dim), (blocks,), jnp.float32, smallest / len(pieces), high / len(pieces)))
        loudness = loudness * jnp.repeat(draws, extent[dim] // blocks).reshape([-1 if axis == dim else 1 for axis in range(len(extent))])
    return loudness


def scatter_about(key, extent, spread, limit, shards=(), dtype=jnp.bfloat16):
    values = spread * jax.random.normal(key, extent, jnp.float32)
    if shards:
        values = values * block_scale(key, extent, shards, -0.22, 0.18)
    return jnp.clip(values, -limit, limit).astype(dtype)


def setup_inputs(seed: int = 0) -> dict:
    seeds = jax.random.split(jax.random.key(seed), 16)
    inputs = scatter_about(seeds[0], (TOKENS, D), 1.0, 6.0, ((0, 16), (1, 2)))
    value_cotangent = scatter_about(seeds[1], (TOKENS, H * VD), 1.0, 6.0, ((0, 16), (1, 2)))
    first_map = scatter_about(seeds[2], (TOKENS, H * VD), 1.0, 6.0, ((0, 16), (1, 2)))
    second_map = scatter_about(seeds[3], (TOKENS, H * VD), 1.0, 6.0, ((0, 16), (1, 2)))
    lambdas = jnp.clip(0.3 + 0.5 * jax.random.uniform(seeds[4], (H,), jnp.float32) ** block_scale(seeds[4], (H,), ((0, 2),), -0.2, 0.2), 0.3, 0.8)
    head_gain = jnp.clip(1.0 + 0.18 * jax.random.normal(seeds[5], (VD,), jnp.float32), 0.1, 1.9)
    output_cotangent = scatter_about(seeds[6], (TOKENS, D), 1.0, 6.0, ((0, 16), (1, 2)))
    value_factor = scatter_about(seeds[7], (D, R), D ** -0.5, 0.125)
    output_factor = scatter_about(seeds[8], (D, R), D ** -0.5, 0.125)
    value_weight = scatter_about(seeds[9], (D, H * VD), D ** -0.5, 0.125, ((0, 16), (1, 2)), jnp.float32)
    output_weight = scatter_about(seeds[10], (H * VD, D), (H * VD) ** -0.5, 0.125, ((0, 2), (1, 16)), jnp.float32)
    value_moment = scatter_about(seeds[11], (R, H * VD), 1.0, 6.0, ((0, 16), (1, 2)), jnp.float32)
    value_second = jnp.clip(jnp.exp(math.log(4.0) - 2.7725887 * jax.random.uniform(seeds[12], (R, H * VD), jnp.float32) ** block_scale(seeds[12], (R, H * VD), ((0, 16), (1, 2)), -0.2, 0.2)), 0.25, 4.0)
    output_moment = scatter_about(seeds[13], (R, H * VD), 1.0, 6.0, ((0, 16), (1, 2)), jnp.float32)
    output_second = jnp.clip(jnp.exp(math.log(4.0) - 2.7725887 * jax.random.uniform(seeds[14], (R, H * VD), jnp.float32) ** block_scale(seeds[14], (R, H * VD), ((0, 16), (1, 2)), -0.2, 0.2)), 0.25, 4.0)
    return {"inputs": inputs, "value_cotangent": value_cotangent, "first_map": first_map, "second_map": second_map, "lambdas": lambdas, "head_gain": head_gain, "output_cotangent": output_cotangent, "value_factor": value_factor, "output_factor": output_factor, "value_weight": value_weight, "output_weight": output_weight, "value_moment": value_moment, "value_second": value_second, "output_moment": output_moment, "output_second": output_second}


def contract_rows(left, right, precise):
    if precise:
        return lax.dot_general(left, right, (((0,), (0,)), ((), ())), precision=lax.Precision.HIGHEST, preferred_element_type=jnp.float32)
    return lax.dot_general(left, right, (((0,), (0,)), ((), ())), preferred_element_type=jnp.float32)

def reference(inputs, value_cotangent, first_map, second_map, lambdas, head_gain, output_cotangent, value_factor, output_factor, value_weight, output_weight, value_moment, value_second, output_moment, output_second):
    tok_count = inputs.shape[0]
    first = first_map.astype(jnp.float32).reshape(tok_count, H, VD)
    second = second_map.astype(jnp.float32).reshape(tok_count, H, VD)
    difference = first - lambdas[None, :, None] * second
    normed = difference * lax.rsqrt(lax.optimization_barrier(jnp.mean(difference * difference, axis=-1, keepdims=True)) + 1e-06) * head_gain
    heads_out = normed.reshape(tok_count, H * VD).astype(jnp.bfloat16)
    token_scale = 1.0 / math.sqrt(TOKENS)
    grad_value = contract_rows(inputs, value_cotangent, False) * token_scale
    grad_output_t = contract_rows(output_cotangent, heads_out, False) * token_scale
    low_value = contract_rows(value_factor.astype(jnp.float32), grad_value, True)
    low_output = contract_rows(output_factor.astype(jnp.float32), grad_output_t, True)
    value_moment_new = 0.8 * value_moment + 0.2 * low_value
    value_second_new = 0.95 * value_second + 0.05 * low_value * low_value
    output_moment_new = 0.8 * output_moment + 0.2 * low_output
    output_second_new = 0.95 * output_second + 0.05 * low_output * low_output
    direction_value = value_moment_new / (jnp.sqrt(value_second_new) + 1e-08)
    direction_output = output_moment_new / (jnp.sqrt(output_second_new) + 1e-08)
    step_value = jnp.dot(value_factor.astype(jnp.float32), direction_value, precision=lax.Precision.HIGHEST, preferred_element_type=jnp.float32)
    step_output = jnp.dot(output_factor.astype(jnp.float32), direction_output, precision=lax.Precision.HIGHEST, preferred_element_type=jnp.float32)
    value_master = value_weight - 0.05 * step_value
    output_master = output_weight - 0.05 * step_output.T
    return (value_master, output_master, value_moment_new, value_second_new, output_moment_new, output_second_new, value_master.astype(jnp.bfloat16), output_master.astype(jnp.bfloat16))
```

```python
import functools
import math

import jax
import jax.numpy as jnp
from jax import lax
from jax.experimental import pallas as pl
from jax.experimental.pallas import tpu as pltpu
from jax.sharding import PartitionSpec as P

F32 = jnp.float32
BF16 = jnp.bfloat16

CODE = 2.0**30
GRAIN = 2.0**40
NX = 2
NY = 2
NC = NX * NY


def encode(w):
    square = (w * CODE) * (w * CODE)
    fourth = square * square
    return jnp.where(w < 0, -fourth, fourth).astype(BF16)


def decode(v):
    v = v.astype(F32)
    size = lax.rsqrt(lax.rsqrt(jnp.maximum(jnp.abs(v), 1e-36))) * (1.0 / CODE)
    return jnp.where(v < 0, -size, size)


def general(nz):
    js = range(1, nz)
    order = [("zf", "v", 1), ("zf", "v", 2), ("rs1", "v"), ("zf", "o", 1), ("zf", "o", 2), ("nf", "v", 0)]
    order += [("rs1", "o"), ("sp", "v", 1, "y"), ("sp", "v", 1, "x"), ("rs2", "v"), ("nf", "o", 0)]
    order += [("sp", "o", 1, "x"), ("sp", "o", 1, "y"), ("rs2", "o")]
    order += [("zf", kind, j) for j in range(3, nz) for kind in ("v", "o")]
    order += [("agz", "v", j) for j in js] + [("agz", "o", j) for j in js]
    order += [("dg", "v"), ("dg", "o")]
    order += [("sp", "v", 2, "y"), ("sp", "v", 2, "x"), ("sp", "o", 2, "x"), ("sp", "o", 2, "y")]
    order += [("agn", kind, j) for kind in ("v", "o") for j in range(nz)]
    order += [("nf", "v", 1), ("nf", "o", 1)]
    for j in range(3, nz):
        order += [("sp", "v", j, "y"), ("sp", "v", j, "x"), ("sp", "o", j, "x"), ("sp", "o", j, "y")]
    order += [("dz", kind, j) for j in (1, 2) for kind in ("v", "o")]
    for kind in ("v", "o"):
        order += [("dirs", kind), ("up", kind, 0, "c"), ("up", kind, 0, "d"), ("nf", kind, 2)]
    order += [("dz", kind, j) for j in range(3, nz) for kind in ("v", "o")]
    for j in js:
        order += [("nf", kind, j) for kind in ("v", "o") if j >= 3]
        order += [("up", kind, j, part) for kind in ("v", "o") for part in ("c", "d")]
    return [
        ("a", "v", "z"), ("a", "o", "z"), ("a", "v", "y"), ("a", "v", "x"),
        ("c", "v"), ("c", "o"), ("a", "o", "x"), ("a", "o", "y"),
    ] + [step for step in order if len(step) < 3 or step[2] < nz]


def squared(g):
    g = g * GRAIN
    return (g * jnp.abs(g)).astype(BF16)


def rooted(v):
    v = v.astype(F32)
    return v * lax.rsqrt(jnp.maximum(jnp.abs(v), 1e-36)) * (1.0 / GRAIN)


def schedule(nz):
    return general(nz)


def exchange(
    nfs, ntp, scale,
    vw_hbm, ow_hbm, inp_hbm, vfac_hbm, ocot_hbm, ofac_hbm, vcot_hbm, first_hbm, second_hbm,
    vm_hbm, vs_hbm, om_hbm, os_hbm, lam_hbm, gain_hbm,
    v_out, o_out, v_master, o_master, vm_new, vs_new, om_new, os_new,
    vw_in, ow_in, inp, vfac, ocot, ofac, vcot, first, second, vm, vs, om, os_, lam, gain,
    gv, go, heads, proj_v, proj_o,
    part_v, part_o, got_v, got_o, sum_v, sum_o, col_v, col_o,
    dfull_v, dfull_o, turned,
    wsend, wrecv, drecv, psend, precv, rsend, rrecv, csend, crecv, asend, arecv, insem,
):
    me = lax.axis_index("fs")
    tp = lax.axis_index("tp")
    tokens, cols = inp.shape
    width = vw_in.shape[0]
    rows = vm.shape[0]
    nz = nfs // NC
    x = lax.rem(me, NX)
    y = lax.rem(lax.div(me, NX), NY)
    z = lax.div(me, NC)
    ox, oy = 1 - x, 1 - y
    cut = {"v": width * 7 // 8 // 16 * 16, "o": cols * 7 // 8 // 16 * 16}
    size = {"v": width, "o": cols}
    index = {"v": 0, "o": 1}
    store = {"v": gv, "o": go}
    flat = len(o_out.shape) == 2

    def at(p, cy, cx):
        return (p * NY + cy) * NX + cx

    below = nz - 1 - z
    pairs = jnp.minimum(z, below)

    def plane(j):
        if j == 0:
            return z
        near = z + (-1 if j % 2 else 1) * ((j + 1) // 2)
        rest = jnp.where(z < below, j, nz - 1 - j)
        return jnp.where(j <= 2 * pairs, near, rest)

    planes = [plane(j) for j in range(nz)]

    def onward(j):
        p = planes[j]
        rising = p < z
        go_on = (rising & (z + 1 < nz)) | (jnp.logical_not(rising) & (z > 0))
        target = at(jnp.where(rising, lax.rem(z + 1, nz), lax.rem(z + nz - 1, nz)), y, x)
        return go_on, target

    barrier = pltpu.get_barrier_semaphore()
    for k in (1, 2, 3):
        pl.semaphore_signal(barrier, inc=1, device_id={"fs": at(z, oy if k & 2 else y, ox if k & 1 else x)})
    for k in range(1, nz):
        pl.semaphore_signal(barrier, inc=1, device_id={"fs": at(lax.rem(z + k, nz), y, x)})
    for k in range(1, ntp):
        pl.semaphore_signal(barrier, inc=1, device_id={"tp": lax.rem(tp + k, ntp)})
    loads = {}
    inputs = {
        "vw": (vw_hbm, vw_in), "ow": (ow_hbm, ow_in), "inp": (inp_hbm, inp), "vfac": (vfac_hbm, vfac),
        "ocot": (ocot_hbm, ocot), "ofac": (ofac_hbm, ofac), "vcot": (vcot_hbm, vcot),
        "first": (first_hbm, first), "second": (second_hbm, second),
        "vm": (vm_hbm, vm), "vs": (vs_hbm, vs), "om": (om_hbm, om), "os": (os_hbm, os_),
        "lam": (lam_hbm, lam), "gain": (gain_hbm, gain),
    }
    for k, (name, (src, dst)) in enumerate(inputs.items()):
        loads[name] = pltpu.make_async_copy(src, dst, insem.at[k])
        loads[name].start()
    loads["vw"].wait()
    gv[me] = encode(vw_in[...])
    loads["ow"].wait()
    go[me] = encode(ow_in[...])
    pl.semaphore_wait(barrier, NC + nz + ntp - 3)

    pending = []
    counts = {}

    def when(cond, run):
        if cond is None:
            run()
        else:
            pl.when(cond)(run)

    def send(sems, kind, src, dst, recv, target, cond=None):
        k = counts.get((id(sems), kind), 0)
        counts[(id(sems), kind)] = k + 1

        def make():
            return pltpu.make_async_remote_copy(
                src_ref=src, dst_ref=dst, send_sem=sems.at[index[kind], k],
                recv_sem=recv, device_id={"fs": target},
            )

        when(cond, lambda: make().start())
        pending.append((cond, make))

    def landed(ref, recv, cond=None):
        when(cond, lambda: pltpu.make_async_remote_copy(
            src_ref=ref, dst_ref=ref, send_sem=wsend.at[0, 0], recv_sem=recv,
            device_id={"fs": at(z, y, ox)},
        ).wait_recv())

    def block(kind, b, part=None):
        ref = store[kind].at[b]
        if part is None:
            return ref, wrecv.at[index[kind], b]
        if part == 0:
            return store[kind].at[b, pl.ds(0, cut[kind])], drecv.at[index[kind], b]
        rest = size[kind] - cut[kind]
        return store[kind].at[b, pl.ds(cut[kind], rest)], wrecv.at[index[kind], b]

    def push(kind, b, target, part=None, cond=None):
        ref, recv = block(kind, b, part)
        send(wsend, kind, ref, ref, recv, target, cond)

    def arrived(kind, b, part=None, cond=None):
        ref, recv = block(kind, b, part)
        landed(ref, recv, cond)

    to_x, to_y = at(z, y, ox), at(z, oy, x)
    up, down = at(lax.rem(z + 1, nz), y, x), at(lax.rem(z + nz - 1, nz), y, x)

    links = {"x": to_x, "y": to_y}

    def own_send(kind, link):
        if link == "z":
            push(kind, me, up, cond=z + 1 < nz)
            push(kind, me, down, cond=z > 0)
        else:
            push(kind, me, links[link])

    mine = pl.ds(pl.multiple_of(tp * cols, cols), cols)
    pcopies = {}

    def project(kind, cot, factor, proj):
        proj[0] = jnp.dot(cot[...], factor[mine, :], preferred_element_type=F32)
        pcopies[kind] = []
        for k in range(1, ntp):
            copy = pltpu.make_async_remote_copy(
                src_ref=proj.at[0], dst_ref=proj.at[k],
                send_sem=psend.at[index[kind], k], recv_sem=precv.at[index[kind], k],
                device_id={"tp": lax.rem(tp + k, ntp)},
            )
            copy.start()
            pcopies[kind].append(copy)

    def contract(a, b):
        return lax.dot_general(a, b, (((0,), (0,)), ((), ())), preferred_element_type=F32)

    def reduce_low(kind, proj, right, part, got):
        for copy in pcopies[kind]:
            copy.wait()
        total = proj[0]
        for k in range(1, ntp):
            total = total + proj[k]
        high = total.astype(BF16)
        low = (total - high.astype(F32)).astype(BF16)
        product = (contract(high, right[...]) + contract(low, right[...])) * scale
        for b in range(nfs):
            part[b % NC, b // NC] = squared(product[b * rows:(b + 1) * rows])
        for k in (1, 2, 3):
            cx = ox if k & 1 else x
            cy = oy if k & 2 else y
            send(rsend, kind, part.at[cy * NX + cx], got.at[k], rrecv.at[index[kind], k], at(z, cy, cx))

    def fetch(*names):
        for name in names:
            loads[name].wait()

    def normalize():
        head_width = gain.shape[1]
        for h in range(cols // head_width):
            span = pl.ds(h * head_width, head_width)
            diff = first[:, span].astype(F32) - lam[h] * second[:, span].astype(F32)
            mean = jnp.mean(diff * diff, axis=-1, keepdims=True)
            heads[:, span] = (diff * lax.rsqrt(mean + 1e-06) * gain[...]).astype(BF16)

    def compute(kind):
        if kind == "v":
            fetch("inp", "vfac")
            project("v", inp, vfac, proj_v)
            fetch("ocot", "ofac")
            project("o", ocot, ofac, proj_o)
            fetch("vcot")
            reduce_low("v", proj_v, vcot, part_v, got_v)
        else:
            fetch("first", "second", "lam", "gain", "vm", "vs", "om", "os")
            normalize()
            reduce_low("o", proj_o, heads, part_o, got_o)

    parts = {"v": (part_v, got_v, sum_v, col_v), "o": (part_o, got_o, sum_o, col_o)}
    moments = {"v": (vm, vs, vm_new, vs_new), "o": (om, os_, om_new, os_new)}
    dfull = {"v": dfull_v, "o": dfull_o}

    def rs1(kind):
        part, got, total, col = parts[kind]
        for k in (1, 2, 3):
            landed(got.at[k], rrecv.at[index[kind], k])
        acc = rooted(part[y * NX + x])
        for k in (1, 2, 3):
            acc = acc + rooted(got[k])
        total[...] = squared(acc)
        for d in range(1, nz):
            peer = lax.rem(z + d, nz)
            send(csend, kind, total.at[peer], col.at[d], crecv.at[index[kind], d], at(peer, y, x))

    def rs2(kind):
        part, got, total, col = parts[kind]
        m_ref, s_ref, m_out, s_out = moments[kind]
        for d in range(1, nz):
            landed(col.at[d], crecv.at[index[kind], d])
        g = rooted(total[z])
        for d in range(1, nz):
            g = g + rooted(col[d])
        m = 0.8 * m_ref[...] + 0.2 * g
        s = 0.95 * s_ref[...] + 0.05 * g * g
        m_out[...] = m
        s_out[...] = s
        dfull[kind][me] = (m / (jnp.sqrt(s) + 1e-08)).astype(BF16)
        for d in range(1, nz):
            apush(kind, me, at(lax.rem(z + d, nz), y, x))
        aspread(kind, me)

    def apush(kind, b, target):
        ref = dfull[kind].at[b]
        send(asend, kind, ref, ref, arecv.at[index[kind], b], target)

    def aspread(kind, b):
        for target in (to_y, to_x) if kind == "v" else (to_x, to_y):
            apush(kind, b, target)

    def alanded(kind, b):
        landed(dfull[kind].at[b], arecv.at[index[kind], b])

    def agz(kind, j):
        b = at(planes[j], y, x)
        alanded(kind, b)
        aspread(kind, b)

    def agn(kind, j):
        b = at(planes[j], oy, x) if kind == "v" else at(planes[j], y, ox)
        alanded(kind, b)
        apush(kind, b, to_x if kind == "v" else to_y)

    def whole(kind):
        d = dfull[kind][...]
        if rows % 16:
            return d.astype(F32).reshape(nfs * rows, cols).astype(BF16)
        return d.reshape(nfs * rows, cols)

    def dirs(kind):
        for p in planes:
            alanded(kind, at(p, y, ox) if kind == "v" else at(p, oy, x))
            alanded(kind, at(p, oy, ox))
        if kind == "o":
            turned[...] = whole(kind).T

    def factor_rows(b, r0, n):
        return pl.ds(pl.multiple_of(b * width + r0, 16), n)

    def move_v(b, r0, n):
        return 0.05 * jnp.dot(vfac[factor_rows(b, r0, n), :], whole("v"), preferred_element_type=F32)

    def move_o(b, r0, n):
        return 0.05 * lax.dot_general(
            turned[pl.ds(r0, n), :], ofac[factor_rows(b, 0, width), :],
            (((1,), (1,)), ((), ())), preferred_element_type=F32,
        )

    def put_o(b, r0, n, new):
        if flat:
            o_out[pl.ds(r0, n), pl.ds(pl.multiple_of(b * width, width), width)] = new
        else:
            o_out[b, pl.ds(r0, n), :] = new

    def refresh(kind, b, r0=0, n=None):
        n = size[kind] - r0 if n is None else n
        if kind == "v":
            old = decode(gv[b, pl.ds(r0, n), :])
            v_out[factor_rows(b, r0, n), :] = (old - move_v(b, r0, n)).astype(BF16)
        else:
            old = decode(go[b, pl.ds(r0, n), :])
            put_o(b, r0, n, (old - move_o(b, r0, n)).astype(BF16))

    def own(kind):
        if kind == "v":
            new = vw_in[...] - move_v(me, 0, width)
            v_master[...] = new
            v_out[factor_rows(me, 0, width), :] = new.astype(BF16)
        else:
            new = ow_in[...] - move_o(me, 0, cols)
            o_master[...] = new
            put_o(me, 0, cols, new.astype(BF16))

    waited = {}

    def await_block(what, kind, j, cond=None):
        p = planes[j]
        b, part = {
            "a": (at(p, y, x), None),
            "n": (at(p, oy, x) if kind == "v" else at(p, y, ox), None),
            "m": (at(p, y, ox) if kind == "v" else at(p, oy, x), None),
            "d": (at(p, oy, ox), 1 if j else None),
            "e": (at(p, oy, ox), 0),
        }[what]
        state = waited.get((what, kind, j))
        if state == "all" or (state == "some" and cond is not None):
            return b
        if state == "some":
            arrived(kind, b, part, jnp.logical_not(onward(j)[0]))
        else:
            arrived(kind, b, part, cond)
        waited[what, kind, j] = "all" if cond is None else "some"
        return b

    def zf(kind, j):
        go_on, target = onward(j)
        push(kind, await_block("a", kind, j, go_on), target, cond=go_on)

    def sp(kind, j, link):
        push(kind, await_block("a", kind, j), links[link])

    def nf(kind, j):
        push(kind, await_block("n", kind, j), to_x if kind == "v" else to_y, 1 if j else None)

    def dg(kind):
        b = await_block("d", kind, 0)
        push(kind, b, up, 0, z + 1 < nz)
        push(kind, b, down, 0, z > 0)

    def dz(kind, j):
        go_on, target = onward(j)
        push(kind, await_block("e", kind, j, go_on), target, 0, go_on)

    def update(kind, j, part):
        p = planes[j]
        if part == "d":
            b = await_block("d", kind, j)
            if j:
                await_block("e", kind, j)
            refresh(kind, b)
            return
        if j:
            await_block("a", kind, j)
        await_block("n", kind, j)
        await_block("m", kind, j)
        if j == 0:
            own(kind)

        def step(c, carry):
            cy = jnp.where(c == 2, oy, y)
            cx = jnp.where(c == 1, ox, x)
            refresh(kind, at(p, cy, cx))
            return carry

        lax.fori_loop(0 if j else 1, 3, step, 0)

    ops = {
        "a": own_send, "c": compute, "zf": zf, "sp": sp, "nf": nf, "dg": dg, "dz": dz,
        "rs1": rs1, "rs2": rs2, "agz": agz, "agn": agn, "dirs": dirs, "up": update,
    }
    for name, *args in schedule(nz):
        ops[name](*args)
    for cond, make in pending:
        when(cond, lambda make=make: make().wait_send())


def publish(count, *refs):
    sems = refs[-1]
    copies = [
        pltpu.make_async_copy(refs[k], refs[count + k], sems.at[k]) for k in range(count)
    ]
    for copy in copies:
        copy.start()
    for copy in copies:
        copy.wait()


def local(
    nfs, ntp,
    inputs, value_cotangent, first_map, second_map, lambdas, head_gain,
    output_cotangent, value_factor, output_factor, value_weight, output_weight,
    value_moment, value_second, output_moment, output_second,
):
    tokens, cols = inputs.shape
    width = value_weight.shape[0]
    rank = value_factor.shape[1]
    rows = value_moment.shape[0]
    nz = nfs // NC
    scale = 1.0 / math.sqrt(tokens * nfs)
    flat = width % 128 == 0
    vmem = pl.BlockSpec(memory_space=pltpu.VMEM)
    hbm = pl.BlockSpec(memory_space=pl.ANY)
    dma = pltpu.SemaphoreType.DMA
    moment = jax.ShapeDtypeStruct((rows, cols), F32)
    out_shape = (
        jax.ShapeDtypeStruct((nfs * width, cols), BF16),
        jax.ShapeDtypeStruct((cols, nfs * width) if flat else (nfs, cols, width), BF16),
        jax.ShapeDtypeStruct((width, cols), F32),
        jax.ShapeDtypeStruct((cols, width), F32),
        moment, moment, moment, moment,
    )
    operands = (
        value_weight, output_weight, inputs, value_factor, output_cotangent, output_factor,
        value_cotangent, first_map, second_map,
        value_moment, value_second, output_moment, output_second, lambdas, head_gain.reshape(1, -1),
    )
    spaces = [pltpu.SMEM if operand is lambdas else pltpu.VMEM for operand in operands]
    shapes = [
        ((nfs, width, cols), BF16),
        ((nfs, cols, width), BF16),
        ((tokens, cols), BF16),
        *[((ntp, tokens, rank), F32)] * 2,
        *[((NC, nz, rows, cols), BF16)] * 4,
        *[((nz, rows, cols), BF16)] * 4,
        *[((nfs, rows, cols), BF16)] * 2,
        ((cols, rank), BF16),
    ]
    sends = 4 + 9 * nz
    outs = pl.pallas_call(
        functools.partial(exchange, nfs, ntp, scale),
        out_shape=tuple(pltpu.VMEM(out.shape, out.dtype) for out in out_shape),
        in_specs=[hbm] * len(operands),
        out_specs=(vmem,) * 8,
        scratch_shapes=[
            *[space(operand.shape, operand.dtype) for space, operand in zip(spaces, operands)],
            *[pltpu.VMEM(shape, dtype) for shape, dtype in shapes],
            dma((2, sends)), dma((2, nfs)), dma((2, nfs)),
            dma((2, ntp)), dma((2, ntp)),
            dma((2, NC)), dma((2, NC)),
            dma((2, nz)), dma((2, nz)),
            dma((2, 5 * nz)), dma((2, nfs)), dma((len(operands),)),
        ],
        compiler_params=pltpu.CompilerParams(collective_id=0, has_side_effects=True, vmem_limit_bytes=VMEM_LIMIT),
    )(
        *[pltpu.with_memory_space_constraint(operand, pltpu.HBM) for operand in operands],
    )
    outs = pl.pallas_call(
        functools.partial(publish, len(outs)),
        out_shape=out_shape,
        in_specs=[vmem] * len(outs),
        out_specs=(hbm,) * len(outs),
        scratch_shapes=[dma((len(outs),))],
        compiler_params=pltpu.CompilerParams(vmem_limit_bytes=VMEM_LIMIT),
    )(*outs)
    value_copy, output_copy, value_master, output_master, *moments = outs
    if not flat:
        output_copy = output_copy.transpose(1, 0, 2).reshape(cols, nfs * width)
    return (value_master, output_master, *moments, value_copy, output_copy)


VMEM_LIMIT = 40 * 1024 * 1024


def solution(mesh):
    both = P("fs", "tp")
    in_specs = (
        both, both, both, both, P("tp"), P(), both, P(), P(), both, P("tp", "fs"),
        both, both, both, both,
    )
    out_specs = (
        both, P("tp", "fs"), both, both, both, both, P(None, "tp"), P("tp", None),
    )
    body = functools.partial(local, mesh.shape["fs"], mesh.shape["tp"])
    return jax.shard_map(
        body, mesh=mesh, in_specs=in_specs, out_specs=out_specs, check_vma=False
    )
```

```python
import functools
import math

import jax
import jax.numpy as jnp
from jax import lax
from jax.experimental import pallas as pl
from jax.experimental.pallas import tpu as pltpu
from jax.sharding import PartitionSpec as P

F32 = jnp.float32
BF16 = jnp.bfloat16

CODE = 2.0**30
GRAIN = 2.0**40
NX = 2
NY = 2
NC = NX * NY


def encode(w):
    square = (w * CODE) * (w * CODE)
    fourth = square * square
    return jnp.where(w < 0, -fourth, fourth).astype(BF16)


def decode(v):
    v = v.astype(F32)
    size = lax.rsqrt(lax.rsqrt(jnp.maximum(jnp.abs(v), 1e-36))) * (1.0 / CODE)
    return jnp.where(v < 0, -size, size)


def general(nz):
    js = range(1, nz)
    order = [("zf", "v", 1), ("zf", "v", 2), ("rs1", "v"), ("zf", "o", 1), ("zf", "o", 2), ("nf", "v", 0)]
    order += [("rs1", "o"), ("sp", "v", 1, "y"), ("sp", "v", 1, "x"), ("rs2", "v"), ("nf", "o", 0)]
    order += [("sp", "o", 1, "x"), ("sp", "o", 1, "y"), ("rs2", "o")]
    order += [("zf", kind, j) for j in range(3, nz) for kind in ("v", "o")]
    order += [("agz", "v", j) for j in js] + [("agz", "o", j) for j in js]
    order += [("dg", "v"), ("dg", "o")]
    order += [("sp", "v", 2, "y"), ("sp", "v", 2, "x"), ("sp", "o", 2, "x"), ("sp", "o", 2, "y")]
    order += [("agn", kind, j) for kind in ("v", "o") for j in range(nz)]
    order += [("nf", "v", 1), ("nf", "o", 1)]
    for j in range(3, nz):
        order += [("sp", "v", j, "y"), ("sp", "v", j, "x"), ("sp", "o", j, "x"), ("sp", "o", j, "y")]
    order += [("dz", kind, j) for j in (1, 2) for kind in ("v", "o")]
    for kind in ("v", "o"):
        order += [("dirs", kind), ("up", kind, 0, "c"), ("up", kind, 0, "d"), ("nf", kind, 2)]
    order += [("dz", kind, j) for j in range(3, nz) for kind in ("v", "o")]
    for j in js:
        order += [("nf", kind, j) for kind in ("v", "o") if j >= 3]
        order += [("up", kind, j, part) for kind in ("v", "o") for part in ("c", "d")]
    return [
        ("a", "v", "z"), ("a", "o", "z"), ("a", "v", "y"), ("a", "v", "x"),
        ("c", "v"), ("c", "o"), ("a", "o", "x"), ("a", "o", "y"),
    ] + [step for step in order if len(step) < 3 or step[2] < nz]


def squared(g):
    g = g * GRAIN
    return (g * jnp.abs(g)).astype(BF16)


def rooted(v):
    v = v.astype(F32)
    return v * lax.rsqrt(jnp.maximum(jnp.abs(v), 1e-36)) * (1.0 / GRAIN)


STEPS = (
    ("a", "v", "x"), ("a", "o", "z"), ("a", "v", "y"), ("a", "v", "z"), ("c", "v"), ("zf", "o", 2),
    ("zf", "o", 1), ("a", "o", "x"), ("sp", "v", 1, "y"), ("rs1", "v"), ("c", "o"), ("sp", "o", 1, "x"),
    ("sp", "o", 2, "y"), ("nf", "v", 0), ("zf", "v", 1), ("rs2", "v"), ("zf", "v", 2), ("rs1", "o"),
    ("agz", "v", 1), ("sp", "v", 2, "y"), ("agz", "v", 2), ("nf", "o", 0), ("rs2", "o"), ("zf", "v", 3),
    ("dg", "v"), ("agz", "v", 3), ("agz", "o", 1), ("zf", "o", 3), ("a", "o", "y"), ("agn", "o", 0),
    ("sp", "o", 2, "x"), ("nf", "v", 1), ("agz", "o", 2), ("nf", "v", 2), ("agz", "o", 3), ("agn", "v", 1),
    ("dz", "v", 1), ("nf", "o", 2), ("agn", "v", 3), ("agn", "o", 1), ("nf", "o", 1), ("agn", "v", 0),
    ("agn", "v", 2), ("dg", "o"), ("sp", "v", 2, "x"), ("dirs", "v"), ("dz", "v", 2), ("agn", "o", 3),
    ("agn", "o", 2), ("up", "v", 0, "c"), ("sp", "o", 1, "y"), ("sp", "o", 3, "x"), ("dirs", "o"),
    ("up", "o", 0, "d"), ("sp", "v", 1, "x"), ("sp", "v", 3, "y"), ("up", "o", 1, "d"), ("up", "v", 1, "d"),
    ("dz", "o", 1), ("dz", "o", 2), ("up", "v", 2, "d"), ("up", "v", 2, "c"), ("up", "o", 2, "c"),
    ("nf", "o", 3), ("sp", "o", 3, "y"), ("up", "o", 2, "d"), ("dz", "o", 3), ("dz", "v", 3),
    ("up", "o", 1, "c"), ("sp", "v", 3, "x"), ("up", "v", 0, "d"), ("nf", "v", 3), ("up", "o", 0, "c"),
    ("up", "v", 1, "c"), ("up", "o", 3, "d"), ("up", "o", 3, "c"), ("up", "v", 3, "c"), ("up", "v", 3, "d"),
)


def schedule(nz):
    return STEPS if nz == 4 else general(nz)


def exchange(
    nfs, ntp, scale,
    vw_hbm, ow_hbm, inp_hbm, vfac_hbm, ocot_hbm, ofac_hbm, vcot_hbm, first_hbm, second_hbm,
    vm_hbm, vs_hbm, om_hbm, os_hbm, lam_hbm, gain_hbm,
    v_out, o_out, v_master, o_master, vm_new, vs_new, om_new, os_new,
    vw_in, ow_in, inp, vfac, ocot, ofac, vcot, first, second, vm, vs, om, os_, lam, gain,
    gv, go, heads, proj_v, proj_o,
    part_v, part_o, got_v, got_o, sum_v, sum_o, col_v, col_o,
    dfull_v, dfull_o, turned,
    wsend, wrecv, drecv, psend, precv, rsend, rrecv, csend, crecv, asend, arecv, insem, rising, falling, corner,
):
    me = lax.axis_index("fs")
    tp = lax.axis_index("tp")
    tokens, cols = inp.shape
    width = vw_in.shape[0]
    rows = vm.shape[0]
    nz = nfs // NC
    x = lax.rem(me, NX)
    y = lax.rem(lax.div(me, NX), NY)
    z = lax.div(me, NC)
    ox, oy = 1 - x, 1 - y
    cut = {"v": width * 7 // 8 // 16 * 16, "o": cols * 7 // 8 // 16 * 16}
    size = {"v": width, "o": cols}
    index = {"v": 0, "o": 1}
    store = {"v": gv, "o": go}
    flat = len(o_out.shape) == 2

    def when(cond, run):
        if cond is None:
            run()
        else:
            pl.when(cond)(run)

    def at(p, cy, cx):
        return (p * NY + cy) * NX + cx

    below = nz - 1 - z
    pairs = jnp.minimum(z, below)

    def plane(j):
        if j == 0:
            return z
        near = z + (-1 if j % 2 else 1) * ((j + 1) // 2)
        rest = jnp.where(z < below, j, nz - 1 - j)
        return jnp.where(j <= 2 * pairs, near, rest)

    planes = [plane(j) for j in range(nz)]

    def onward(j):
        p = planes[j]
        rising = p < z
        go_on = (rising & (z + 1 < nz)) | (jnp.logical_not(rising) & (z > 0))
        target = at(jnp.where(rising, lax.rem(z + 1, nz), lax.rem(z + nz - 1, nz)), y, x)
        return go_on, target

    to_x, to_y = at(z, y, ox), at(z, oy, x)
    up, down = at(lax.rem(z + 1, nz), y, x), at(lax.rem(z + nz - 1, nz), y, x)
    has_up, has_down = z + 1 < nz, z > 0
    barrier = pltpu.get_barrier_semaphore()
    for target, cond in ((to_x, None), (to_y, None), (up, has_up), (down, has_down)):
        when(cond, lambda target=target: pl.semaphore_signal(barrier, inc=1, device_id={"fs": target}))
    for k in range(1, ntp):
        pl.semaphore_signal(barrier, inc=1, device_id={"tp": lax.rem(tp + k, ntp)})
    loads = {}
    inputs = {
        "vw": (vw_hbm, vw_in), "ow": (ow_hbm, ow_in), "inp": (inp_hbm, inp), "vfac": (vfac_hbm, vfac),
        "ocot": (ocot_hbm, ocot), "ofac": (ofac_hbm, ofac), "vcot": (vcot_hbm, vcot),
        "first": (first_hbm, first), "second": (second_hbm, second),
        "vm": (vm_hbm, vm), "vs": (vs_hbm, vs), "om": (om_hbm, om), "os": (os_hbm, os_),
        "lam": (lam_hbm, lam), "gain": (gain_hbm, gain),
    }
    for k, (name, (src, dst)) in enumerate(inputs.items()):
        loads[name] = pltpu.make_async_copy(src, dst, insem.at[k])
    first_loads = ("vw", "ow", "inp", "vfac")
    for name in first_loads:
        loads[name].start()
    loads["vw"].wait()
    for name in loads:
        if name not in first_loads:
            loads[name].start()
    gv[me] = encode(vw_in[...])
    loads["ow"].wait()
    go[me] = encode(ow_in[...])
    pl.semaphore_wait(barrier, 1 + ntp + jnp.where(has_up, 1, 0) + jnp.where(has_down, 1, 0))

    def tell(k):
        when(has_up, lambda: pl.semaphore_signal(rising.at[k], inc=1, device_id={"fs": up}))
        when(has_down, lambda: pl.semaphore_signal(falling.at[k], inc=1, device_id={"fs": down}))

    def hear(k):
        when(has_down, lambda: pl.semaphore_wait(rising.at[k], 1))
        when(has_up, lambda: pl.semaphore_wait(falling.at[k], 1))

    pl.semaphore_signal(corner, inc=1, device_id={"fs": to_x})
    steps = max(nz - 2, 0)
    if steps:
        tell(0)

    pending = []
    counts = {}

    def send(sems, kind, src, dst, recv, target, cond=None):
        k = counts.get((id(sems), kind), 0)
        counts[(id(sems), kind)] = k + 1

        def make():
            return pltpu.make_async_remote_copy(
                src_ref=src, dst_ref=dst, send_sem=sems.at[index[kind], k],
                recv_sem=recv, device_id={"fs": target},
            )

        when(cond, lambda: make().start())
        pending.append((cond, make))

    def landed(ref, recv, cond=None):
        when(cond, lambda: pltpu.make_async_remote_copy(
            src_ref=ref, dst_ref=ref, send_sem=wsend.at[0, 0], recv_sem=recv,
            device_id={"fs": at(z, y, ox)},
        ).wait_recv())

    def block(kind, b, part=None):
        ref = store[kind].at[b]
        if part is None:
            return ref, wrecv.at[index[kind], b]
        if part == 0:
            return store[kind].at[b, pl.ds(0, cut[kind])], drecv.at[index[kind], b]
        rest = size[kind] - cut[kind]
        return store[kind].at[b, pl.ds(cut[kind], rest)], wrecv.at[index[kind], b]

    def push(kind, b, target, part=None, cond=None):
        ref, recv = block(kind, b, part)
        send(wsend, kind, ref, ref, recv, target, cond)

    def arrived(kind, b, part=None, cond=None):
        ref, recv = block(kind, b, part)
        landed(ref, recv, cond)

    to_x, to_y = at(z, y, ox), at(z, oy, x)
    up, down = at(lax.rem(z + 1, nz), y, x), at(lax.rem(z + nz - 1, nz), y, x)

    links = {"x": to_x, "y": to_y}

    def own_send(kind, link):
        if link == "z":
            push(kind, me, up, cond=has_up)
            push(kind, me, down, cond=has_down)
        else:
            push(kind, me, links[link])

    mine = pl.ds(pl.multiple_of(tp * cols, cols), cols)
    pcopies = {}

    def project(kind, cot, factor, proj):
        proj[0] = jnp.dot(cot[...], factor[mine, :], preferred_element_type=F32)
        pcopies[kind] = []
        for k in range(1, ntp):
            copy = pltpu.make_async_remote_copy(
                src_ref=proj.at[0], dst_ref=proj.at[k],
                send_sem=psend.at[index[kind], k], recv_sem=precv.at[index[kind], k],
                device_id={"tp": lax.rem(tp + k, ntp)},
            )
            copy.start()
            pcopies[kind].append(copy)

    def contract(a, b):
        return lax.dot_general(a, b, (((0,), (0,)), ((), ())), preferred_element_type=F32)

    def reduce_low(kind, proj, right, part, got):
        for copy in pcopies[kind]:
            copy.wait()
        total = proj[0]
        for k in range(1, ntp):
            total = total + proj[k]
        high = total.astype(BF16)
        low = (total - high.astype(F32)).astype(BF16)
        product = (contract(high, right[...]) + contract(low, right[...])) * scale
        for b in range(nfs):
            part[b % NC, b // NC] = squared(product[b * rows:(b + 1) * rows])
        for k in (1, 2, 3):
            cx = ox if k & 1 else x
            cy = oy if k & 2 else y
            send(rsend, kind, part.at[cy * NX + cx], got.at[k], rrecv.at[index[kind], k], at(z, cy, cx))

    def fetch(*names):
        for name in names:
            loads[name].wait()

    def normalize():
        head_width = gain.shape[1]
        for h in range(cols // head_width):
            span = pl.ds(h * head_width, head_width)
            diff = first[:, span].astype(F32) - lam[h] * second[:, span].astype(F32)
            mean = jnp.mean(diff * diff, axis=-1, keepdims=True)
            heads[:, span] = (diff * lax.rsqrt(mean + 1e-06) * gain[...]).astype(BF16)

    def compute(kind):
        if kind == "v":
            fetch("inp", "vfac")
            project("v", inp, vfac, proj_v)
            fetch("ocot", "ofac")
            project("o", ocot, ofac, proj_o)
            fetch("vcot")
            pl.semaphore_wait(corner, 1)
            for k in range(1, steps):
                hear(k - 1)
                tell(k)
            reduce_low("v", proj_v, vcot, part_v, got_v)
        else:
            fetch("first", "second", "lam", "gain", "vm", "vs", "om", "os")
            normalize()
            reduce_low("o", proj_o, heads, part_o, got_o)

    parts = {"v": (part_v, got_v, sum_v, col_v), "o": (part_o, got_o, sum_o, col_o)}
    moments = {"v": (vm, vs, vm_new, vs_new), "o": (om, os_, om_new, os_new)}
    dfull = {"v": dfull_v, "o": dfull_o}

    heard = []

    def rs1(kind):
        part, got, total, col = parts[kind]
        if steps and not heard:
            hear(steps - 1)
            heard.append(True)
        for k in (1, 2, 3):
            landed(got.at[k], rrecv.at[index[kind], k])
        acc = rooted(part[y * NX + x])
        for k in (1, 2, 3):
            acc = acc + rooted(got[k])
        total[...] = squared(acc)
        for d in range(1, nz):
            peer = lax.rem(z + d, nz)
            send(csend, kind, total.at[peer], col.at[d], crecv.at[index[kind], d], at(peer, y, x))

    def rs2(kind):
        part, got, total, col = parts[kind]
        m_ref, s_ref, m_out, s_out = moments[kind]
        for d in range(1, nz):
            landed(col.at[d], crecv.at[index[kind], d])
        g = rooted(total[z])
        for d in range(1, nz):
            g = g + rooted(col[d])
        m = 0.8 * m_ref[...] + 0.2 * g
        s = 0.95 * s_ref[...] + 0.05 * g * g
        m_out[...] = m
        s_out[...] = s
        dfull[kind][me] = (m / (jnp.sqrt(s) + 1e-08)).astype(BF16)
        for d in range(1, nz):
            apush(kind, me, at(lax.rem(z + d, nz), y, x))
        aspread(kind, me)

    def apush(kind, b, target):
        ref = dfull[kind].at[b]
        send(asend, kind, ref, ref, arecv.at[index[kind], b], target)

    def aspread(kind, b):
        for target in (to_y, to_x) if kind == "v" else (to_x, to_y):
            apush(kind, b, target)

    def alanded(kind, b):
        landed(dfull[kind].at[b], arecv.at[index[kind], b])

    def agz(kind, j):
        b = at(planes[j], y, x)
        alanded(kind, b)
        aspread(kind, b)

    def agn(kind, j):
        b = at(planes[j], oy, x) if kind == "v" else at(planes[j], y, ox)
        alanded(kind, b)
        apush(kind, b, to_x if kind == "v" else to_y)

    def whole(kind):
        d = dfull[kind][...]
        if rows % 16:
            return d.astype(F32).reshape(nfs * rows, cols).astype(BF16)
        return d.reshape(nfs * rows, cols)

    def dirs(kind):
        for p in planes:
            alanded(kind, at(p, y, ox) if kind == "v" else at(p, oy, x))
            alanded(kind, at(p, oy, ox))
        if kind == "o":
            turned[...] = whole(kind).T

    def factor_rows(b, r0, n):
        return pl.ds(pl.multiple_of(b * width + r0, 16), n)

    def move_v(b, r0, n):
        return 0.05 * jnp.dot(vfac[factor_rows(b, r0, n), :], whole("v"), preferred_element_type=F32)

    def move_o(b, r0, n):
        return 0.05 * lax.dot_general(
            turned[pl.ds(r0, n), :], ofac[factor_rows(b, 0, width), :],
            (((1,), (1,)), ((), ())), preferred_element_type=F32,
        )

    def put_o(b, r0, n, new):
        if flat:
            o_out[pl.ds(r0, n), pl.ds(pl.multiple_of(b * width, width), width)] = new
        else:
            o_out[b, pl.ds(r0, n), :] = new

    def refresh(kind, b, r0=0, n=None):
        n = size[kind] - r0 if n is None else n
        if kind == "v":
            old = decode(gv[b, pl.ds(r0, n), :])
            v_out[factor_rows(b, r0, n), :] = (old - move_v(b, r0, n)).astype(BF16)
        else:
            old = decode(go[b, pl.ds(r0, n), :])
            put_o(b, r0, n, (old - move_o(b, r0, n)).astype(BF16))

    def own(kind):
        if kind == "v":
            new = vw_in[...] - move_v(me, 0, width)
            v_master[...] = new
            v_out[factor_rows(me, 0, width), :] = new.astype(BF16)
        else:
            new = ow_in[...] - move_o(me, 0, cols)
            o_master[...] = new
            put_o(me, 0, cols, new.astype(BF16))

    waited = {}

    def await_block(what, kind, j, cond=None):
        p = planes[j]
        b, part = {
            "a": (at(p, y, x), None),
            "n": (at(p, oy, x) if kind == "v" else at(p, y, ox), None),
            "m": (at(p, y, ox) if kind == "v" else at(p, oy, x), None),
            "d": (at(p, oy, ox), 1 if j else None),
            "e": (at(p, oy, ox), 0),
        }[what]
        state = waited.get((what, kind, j))
        if state == "all" or (state == "some" and cond is not None):
            return b
        if state == "some":
            arrived(kind, b, part, jnp.logical_not(onward(j)[0]))
        else:
            arrived(kind, b, part, cond)
        waited[what, kind, j] = "all" if cond is None else "some"
        return b

    def zf(kind, j):
        go_on, target = onward(j)
        push(kind, await_block("a", kind, j, go_on), target, cond=go_on)

    def sp(kind, j, link):
        push(kind, await_block("a", kind, j), links[link])

    def nf(kind, j):
        push(kind, await_block("n", kind, j), to_x if kind == "v" else to_y, 1 if j else None)

    def dg(kind):
        b = await_block("d", kind, 0)
        push(kind, b, up, 0, has_up)
        push(kind, b, down, 0, has_down)

    def dz(kind, j):
        go_on, target = onward(j)
        push(kind, await_block("e", kind, j, go_on), target, 0, go_on)

    def update(kind, j, part):
        p = planes[j]
        if part == "d":
            b = await_block("d", kind, j)
            if j:
                await_block("e", kind, j)
            refresh(kind, b)
            return
        if j:
            await_block("a", kind, j)
        await_block("n", kind, j)
        await_block("m", kind, j)
        if j == 0:
            own(kind)

        def step(c, carry):
            cy = jnp.where(c == 2, oy, y)
            cx = jnp.where(c == 1, ox, x)
            refresh(kind, at(p, cy, cx))
            return carry

        lax.fori_loop(0 if j else 1, 3, step, 0)

    ops = {
        "a": own_send, "c": compute, "zf": zf, "sp": sp, "nf": nf, "dg": dg, "dz": dz,
        "rs1": rs1, "rs2": rs2, "agz": agz, "agn": agn, "dirs": dirs, "up": update,
    }
    for name, *args in schedule(nz):
        ops[name](*args)
    for cond, make in pending:
        when(cond, lambda make=make: make().wait_send())


def publish(count, *refs):
    sems = refs[-1]
    copies = [
        pltpu.make_async_copy(refs[k], refs[count + k], sems.at[k]) for k in range(count)
    ]
    for copy in copies:
        copy.start()
    for copy in copies:
        copy.wait()


def local(
    nfs, ntp,
    inputs, value_cotangent, first_map, second_map, lambdas, head_gain,
    output_cotangent, value_factor, output_factor, value_weight, output_weight,
    value_moment, value_second, output_moment, output_second,
):
    tokens, cols = inputs.shape
    width = value_weight.shape[0]
    rank = value_factor.shape[1]
    rows = value_moment.shape[0]
    nz = nfs // NC
    scale = 1.0 / math.sqrt(tokens * nfs)
    flat = width % 128 == 0
    vmem = pl.BlockSpec(memory_space=pltpu.VMEM)
    hbm = pl.BlockSpec(memory_space=pl.ANY)
    dma = pltpu.SemaphoreType.DMA
    regular = pltpu.SemaphoreType.REGULAR
    moment = jax.ShapeDtypeStruct((rows, cols), F32)
    out_shape = (
        jax.ShapeDtypeStruct((nfs * width, cols), BF16),
        jax.ShapeDtypeStruct((cols, nfs * width) if flat else (nfs, cols, width), BF16),
        jax.ShapeDtypeStruct((width, cols), F32),
        jax.ShapeDtypeStruct((cols, width), F32),
        moment, moment, moment, moment,
    )
    operands = (
        value_weight, output_weight, inputs, value_factor, output_cotangent, output_factor,
        value_cotangent, first_map, second_map,
        value_moment, value_second, output_moment, output_second, lambdas, head_gain.reshape(1, -1),
    )
    spaces = [pltpu.SMEM if operand is lambdas else pltpu.VMEM for operand in operands]
    shapes = [
        ((nfs, width, cols), BF16),
        ((nfs, cols, width), BF16),
        ((tokens, cols), BF16),
        *[((ntp, tokens, rank), F32)] * 2,
        *[((NC, nz, rows, cols), BF16)] * 4,
        *[((nz, rows, cols), BF16)] * 4,
        *[((nfs, rows, cols), BF16)] * 2,
        ((cols, rank), BF16),
    ]
    sends = 4 + 9 * nz
    outs = pl.pallas_call(
        functools.partial(exchange, nfs, ntp, scale),
        out_shape=tuple(pltpu.VMEM(out.shape, out.dtype) for out in out_shape),
        in_specs=[hbm] * len(operands),
        out_specs=(vmem,) * 8,
        scratch_shapes=[
            *[space(operand.shape, operand.dtype) for space, operand in zip(spaces, operands)],
            *[pltpu.VMEM(shape, dtype) for shape, dtype in shapes],
            dma((2, sends)), dma((2, nfs)), dma((2, nfs)),
            dma((2, ntp)), dma((2, ntp)),
            dma((2, NC)), dma((2, NC)),
            dma((2, nz)), dma((2, nz)),
            dma((2, 5 * nz)), dma((2, nfs)), dma((len(operands),)),
            regular((max(nz - 2, 1),)), regular((max(nz - 2, 1),)), regular,
        ],
        compiler_params=pltpu.CompilerParams(collective_id=0, has_side_effects=True, vmem_limit_bytes=VMEM_LIMIT),
    )(
        *[pltpu.with_memory_space_constraint(operand, pltpu.HBM) for operand in operands],
    )
    outs = pl.pallas_call(
        functools.partial(publish, len(outs)),
        out_shape=out_shape,
        in_specs=[vmem] * len(outs),
        out_specs=(hbm,) * len(outs),
        scratch_shapes=[dma((len(outs),))],
        compiler_params=pltpu.CompilerParams(vmem_limit_bytes=VMEM_LIMIT),
    )(*outs)
    value_copy, output_copy, value_master, output_master, *moments = outs
    if not flat:
        output_copy = output_copy.transpose(1, 0, 2).reshape(cols, nfs * width)
    return (value_master, output_master, *moments, value_copy, output_copy)


VMEM_LIMIT = 40 * 1024 * 1024


def solution(mesh):
    both = P("fs", "tp")
    in_specs = (
        both, both, both, both, P("tp"), P(), both, P(), P(), both, P("tp", "fs"),
        both, both, both, both,
    )
    out_specs = (
        both, P("tp", "fs"), both, both, both, both, P(None, "tp"), P("tp", None),
    )
    body = functools.partial(local, mesh.shape["fs"], mesh.shape["tp"])
    return jax.shard_map(
        body, mesh=mesh, in_specs=in_specs, out_specs=out_specs, check_vma=False
    )
```

```python
import functools
import math

import jax
import jax.numpy as jnp
from jax import lax
from jax.experimental import pallas as pl
from jax.experimental.pallas import tpu as pltpu
from jax.sharding import PartitionSpec as P

F32 = jnp.float32
BF16 = jnp.bfloat16

CODE = 2.0**30
GRAIN = 2.0**40
NX = 2
NY = 2
NC = NX * NY


def encode(w):
    square = (w * CODE) * (w * CODE)
    fourth = square * square
    return jnp.where(w < 0, -fourth, fourth).astype(BF16)


def decode(v):
    v = v.astype(F32)
    size = lax.rsqrt(lax.rsqrt(jnp.maximum(jnp.abs(v), 1e-36))) * (1.0 / CODE)
    return jnp.where(v < 0, -size, size)


def general(nz):
    js = range(1, nz)
    order = [("zf", "v", 1), ("zf", "v", 2), ("ra", "v"), ("rs1", "v"), ("zf", "o", 1), ("zf", "o", 2), ("nf", "v", 0)]
    order += [("ra", "o"), ("rs1", "o"), ("sp", "v", 1, "y"), ("sp", "v", 1, "x"), ("rs2", "v"), ("nf", "o", 0)]
    order += [("sp", "o", 1, "x"), ("sp", "o", 1, "y"), ("rs2", "o")]
    order += [("zf", kind, j) for j in range(3, nz) for kind in ("v", "o")]
    order += [("agz", "v", j) for j in js] + [("agz", "o", j) for j in js]
    order += [("dg", "v"), ("dg", "o")]
    order += [("sp", "v", 2, "y"), ("sp", "v", 2, "x"), ("sp", "o", 2, "x"), ("sp", "o", 2, "y")]
    order += [("agn", kind, j) for kind in ("v", "o") for j in range(nz)]
    order += [("nf", "v", 1), ("nf", "o", 1)]
    for j in range(3, nz):
        order += [("sp", "v", j, "y"), ("sp", "v", j, "x"), ("sp", "o", j, "x"), ("sp", "o", j, "y")]
    order += [("dz", kind, j) for j in (1, 2) for kind in ("v", "o")]
    for kind in ("v", "o"):
        order += [("dirs", kind), ("up", kind, 0, "c"), ("up", kind, 0, "d"), ("nf", kind, 2)]
    order += [("dz", kind, j) for j in range(3, nz) for kind in ("v", "o")]
    for j in js:
        order += [("nf", kind, j) for kind in ("v", "o") if j >= 3]
        order += [("up", kind, j, part) for kind in ("v", "o") for part in ("c", "d")]
    return [
        ("a", "v", "z"), ("a", "o", "z"), ("a", "v", "y"), ("a", "v", "x"),
        ("c", "v"), ("c", "o"), ("a", "o", "x"), ("a", "o", "y"),
    ] + [step for step in order if len(step) < 3 or step[2] < nz]


def squared(g):
    g = g * GRAIN
    return (g * jnp.abs(g)).astype(BF16)


def rooted(v):
    v = v.astype(F32)
    return v * lax.rsqrt(jnp.maximum(jnp.abs(v), 1e-36)) * (1.0 / GRAIN)


STEPS = (
    ("a", "v", "y"), ("a", "o", "z"), ("a", "o", "x"), ("c", "v"), ("a", "v", "z"), ("c", "o"),
    ("nf", "v", 0), ("ra", "v"), ("sp", "o", 1, "x"), ("nf", "o", 0), ("zf", "o", 1), ("zf", "o", 2),
    ("rs1", "v"), ("zf", "v", 2), ("zf", "v", 1), ("sp", "o", 1, "y"), ("ra", "o"), ("sp", "v", 2, "y"),
    ("sp", "o", 2, "x"), ("sp", "o", 2, "y"), ("sp", "v", 1, "y"), ("rs2", "v"), ("rs1", "o"), ("zf", "o", 3),
    ("zf", "v", 3), ("sp", "v", 2, "x"), ("rs2", "o"), ("agz", "v", 1), ("sp", "v", 1, "x"), ("dg", "o"),
    ("agz", "v", 3), ("nf", "v", 1), ("agz", "o", 1), ("dz", "o", 1), ("dg", "v"), ("agn", "o", 0),
    ("agz", "v", 2), ("agz", "o", 2), ("dz", "o", 2), ("nf", "o", 1), ("agz", "o", 3), ("agn", "v", 3),
    ("agn", "v", 0), ("sp", "v", 3, "y"), ("dz", "v", 2), ("agn", "v", 1), ("nf", "v", 2), ("nf", "o", 2),
    ("agn", "o", 2), ("dz", "v", 1), ("dz", "o", 3), ("agn", "v", 2), ("sp", "o", 3, "x"),
    ("sp", "v", 3, "x"), ("agn", "o", 3), ("dz", "v", 3), ("dirs", "v"), ("up", "v", 1, "c"), ("agn", "o", 1),
    ("up", "v", 1, "d"), ("nf", "o", 3), ("a", "o", "y"), ("dirs", "o"), ("sp", "o", 3, "y"),
    ("up", "o", 0, "d"), ("up", "o", 2, "c"), ("up", "o", 1, "c"), ("a", "v", "x"), ("up", "v", 2, "c"),
    ("up", "v", 0, "d"), ("up", "o", 1, "d"), ("up", "v", 3, "c"), ("up", "o", 2, "d"), ("nf", "v", 3),
    ("up", "o", 3, "d"), ("up", "v", 2, "d"), ("up", "o", 0, "c"), ("up", "v", 0, "c"), ("up", "o", 3, "c"),
    ("up", "v", 3, "d"),
)


def schedule(nz):
    return STEPS if nz == 4 else general(nz)


def exchange(
    nfs, ntp, scale,
    vw_hbm, ow_hbm, inp_hbm, vfac_hbm, ocot_hbm, ofac_hbm, vcot_hbm, first_hbm, second_hbm,
    vm_hbm, vs_hbm, om_hbm, os_hbm, lam_hbm, gain_hbm,
    v_out, o_out, v_master, o_master, vm_new, vs_new, om_new, os_new,
    vw_in, ow_in, inp, vfac, ocot, ofac, vcot, first, second, vm, vs, om, os_, lam, gain,
    gv, go, heads, proj_v, proj_o,
    part_v, part_o, got_v, got_o, mid_v, mid_o, half_v, half_o, sum_v, sum_o, col_v, col_o, keep_v, keep_o,
    dfull_v, dfull_o, turned,
    wsend, wrecv, drecv, psend, precv, rsend, rrecv, csend, crecv, asend, arecv, insem, rising, falling,
):
    me = lax.axis_index("fs")
    tp = lax.axis_index("tp")
    tokens, cols = inp.shape
    width = vw_in.shape[0]
    rows = vm.shape[0]
    nz = nfs // NC
    x = lax.rem(me, NX)
    y = lax.rem(lax.div(me, NX), NY)
    z = lax.div(me, NC)
    ox, oy = 1 - x, 1 - y
    cut = {"v": width * 7 // 8 // 16 * 16, "o": cols * 13 // 16 // 16 * 16}
    size = {"v": width, "o": cols}
    index = {"v": 0, "o": 1}
    store = {"v": gv, "o": go}
    flat = len(o_out.shape) == 2

    def when(cond, run):
        if cond is None:
            run()
        else:
            pl.when(cond)(run)

    def at(p, cy, cx):
        return (p * NY + cy) * NX + cx

    below = nz - 1 - z
    pairs = jnp.minimum(z, below)

    def plane(j):
        if j == 0:
            return z
        near = z + (-1 if j % 2 else 1) * ((j + 1) // 2)
        rest = jnp.where(z < below, j, nz - 1 - j)
        return jnp.where(j <= 2 * pairs, near, rest)

    planes = [plane(j) for j in range(nz)]

    def onward(j):
        p = planes[j]
        rising = p < z
        go_on = (rising & (z + 1 < nz)) | (jnp.logical_not(rising) & (z > 0))
        target = at(jnp.where(rising, lax.rem(z + 1, nz), lax.rem(z + nz - 1, nz)), y, x)
        return go_on, target

    to_x, to_y = at(z, y, ox), at(z, oy, x)
    up, down = at(lax.rem(z + 1, nz), y, x), at(lax.rem(z + nz - 1, nz), y, x)
    has_up, has_down = z + 1 < nz, z > 0
    barrier = pltpu.get_barrier_semaphore()
    for target, cond in ((to_x, None), (to_y, None), (up, has_up), (down, has_down)):
        when(cond, lambda target=target: pl.semaphore_signal(barrier, inc=1, device_id={"fs": target}))
    for k in range(1, ntp):
        pl.semaphore_signal(barrier, inc=1, device_id={"tp": lax.rem(tp + k, ntp)})
    loads = {}
    inputs = {
        "vw": (vw_hbm, vw_in), "ow": (ow_hbm, ow_in), "inp": (inp_hbm, inp), "vfac": (vfac_hbm, vfac),
        "ocot": (ocot_hbm, ocot), "ofac": (ofac_hbm, ofac), "vcot": (vcot_hbm, vcot),
        "first": (first_hbm, first), "second": (second_hbm, second),
        "vm": (vm_hbm, vm), "vs": (vs_hbm, vs), "om": (om_hbm, om), "os": (os_hbm, os_),
        "lam": (lam_hbm, lam), "gain": (gain_hbm, gain),
    }
    for k, (name, (src, dst)) in enumerate(inputs.items()):
        loads[name] = pltpu.make_async_copy(src, dst, insem.at[k])
    first_loads = ("vw", "ow", "inp", "vfac")
    for name in first_loads:
        loads[name].start()
    loads["vw"].wait()
    for name in loads:
        if name not in first_loads:
            loads[name].start()
    gv[me] = encode(vw_in[...])
    loads["ow"].wait()
    go[me] = encode(ow_in[...])
    pl.semaphore_wait(barrier, 1 + ntp + jnp.where(has_up, 1, 0) + jnp.where(has_down, 1, 0))

    def tell(k):
        when(has_up, lambda: pl.semaphore_signal(rising.at[k], inc=1, device_id={"fs": up}))
        when(has_down, lambda: pl.semaphore_signal(falling.at[k], inc=1, device_id={"fs": down}))

    def hear(k):
        when(has_down, lambda: pl.semaphore_wait(rising.at[k], 1))
        when(has_up, lambda: pl.semaphore_wait(falling.at[k], 1))

    steps = max(nz - 2, 0)
    if steps:
        tell(0)

    pending = []
    counts = {}

    def send(sems, kind, src, dst, recv, target, cond=None):
        k = counts.get((id(sems), kind), 0)
        counts[(id(sems), kind)] = k + 1

        def make():
            return pltpu.make_async_remote_copy(
                src_ref=src, dst_ref=dst, send_sem=sems.at[index[kind], k],
                recv_sem=recv, device_id={"fs": target},
            )

        when(cond, lambda: make().start())
        pending.append((cond, make))

    def landed(ref, recv, cond=None):
        when(cond, lambda: pltpu.make_async_remote_copy(
            src_ref=ref, dst_ref=ref, send_sem=wsend.at[0, 0], recv_sem=recv,
            device_id={"fs": at(z, y, ox)},
        ).wait_recv())

    def block(kind, b, part=None):
        ref = store[kind].at[b]
        if part is None:
            return ref, wrecv.at[index[kind], b]
        if part == 0:
            return store[kind].at[b, pl.ds(0, cut[kind])], drecv.at[index[kind], b]
        rest = size[kind] - cut[kind]
        return store[kind].at[b, pl.ds(cut[kind], rest)], wrecv.at[index[kind], b]

    def push(kind, b, target, part=None, cond=None):
        ref, recv = block(kind, b, part)
        send(wsend, kind, ref, ref, recv, target, cond)

    def arrived(kind, b, part=None, cond=None):
        ref, recv = block(kind, b, part)
        landed(ref, recv, cond)

    to_x, to_y = at(z, y, ox), at(z, oy, x)
    up, down = at(lax.rem(z + 1, nz), y, x), at(lax.rem(z + nz - 1, nz), y, x)

    links = {"x": to_x, "y": to_y}

    def own_send(kind, link):
        if link == "z":
            push(kind, me, up, cond=has_up)
            push(kind, me, down, cond=has_down)
        else:
            push(kind, me, links[link])

    mine = pl.ds(pl.multiple_of(tp * cols, cols), cols)
    pcopies = {}

    def project(kind, cot, factor, proj):
        proj[0] = jnp.dot(cot[...], factor[mine, :], preferred_element_type=F32)
        pcopies[kind] = []
        for k in range(1, ntp):
            copy = pltpu.make_async_remote_copy(
                src_ref=proj.at[0], dst_ref=proj.at[k],
                send_sem=psend.at[index[kind], k], recv_sem=precv.at[index[kind], k],
                device_id={"tp": lax.rem(tp + k, ntp)},
            )
            copy.start()
            pcopies[kind].append(copy)

    def contract(a, b):
        return lax.dot_general(a, b, (((0,), (0,)), ((), ())), preferred_element_type=F32)

    def reduce_low(kind, proj, right, part, got):
        for copy in pcopies[kind]:
            copy.wait()
        total = proj[0]
        for k in range(1, ntp):
            total = total + proj[k]
        high = total.astype(BF16)
        low = (total - high.astype(F32)).astype(BF16)
        product = (contract(high, right[...]) + contract(low, right[...])) * scale
        for b in range(nfs):
            cy, cx = b // NX % NY, b % NX
            lead, follow = (cx, cy) if kind == "v" else (cy, cx)
            part[lead, follow, b // NC] = squared(product[b * rows:(b + 1) * rows])
        other, target = (ox, to_x) if kind == "v" else (oy, to_y)
        send(rsend, kind, part.at[other], got, rrecv.at[index[kind], 0], target)

    def fetch(*names):
        for name in names:
            loads[name].wait()

    def normalize():
        head_width = gain.shape[1]
        for h in range(cols // head_width):
            span = pl.ds(h * head_width, head_width)
            diff = first[:, span].astype(F32) - lam[h] * second[:, span].astype(F32)
            mean = jnp.mean(diff * diff, axis=-1, keepdims=True)
            heads[:, span] = (diff * lax.rsqrt(mean + 1e-06) * gain[...]).astype(BF16)

    def project_once(kind):
        if kind in pcopies:
            return
        if kind == "v":
            fetch("inp", "vfac")
            project("v", inp, vfac, proj_v)
        else:
            fetch("ocot", "ofac")
            project("o", ocot, ofac, proj_o)

    def compute(kind):
        opening = not pcopies
        project_once(kind)
        project_once("o" if kind == "v" else "v")
        if kind == "v":
            fetch("vcot")
        else:
            fetch("first", "second", "lam", "gain", "vm", "vs", "om", "os")
            normalize()
        if opening:
            for k in range(1, steps):
                hear(k - 1)
                tell(k)
        if kind == "v":
            reduce_low("v", proj_v, vcot, part_v, got_v)
        else:
            reduce_low("o", proj_o, heads, part_o, got_o)

    parts = {
        "v": (part_v, got_v, mid_v, half_v, sum_v, col_v, keep_v),
        "o": (part_o, got_o, mid_o, half_o, sum_o, col_o, keep_o),
    }
    moments = {"v": (vm, vs, vm_new, vs_new), "o": (om, os_, om_new, os_new)}
    dfull = {"v": dfull_v, "o": dfull_o}

    heard = []

    def ra(kind):
        part, got, mid, half, total, col, keep = parts[kind]
        landed(got, rrecv.at[index[kind], 0])
        lead, own, other, target = (x, y, oy, to_y) if kind == "v" else (y, x, ox, to_x)
        keep[...] = rooted(part[lead, own]) + rooted(got[own])
        mid[...] = squared(rooted(part[lead, other]) + rooted(got[other]))
        send(rsend, kind, mid, half, rrecv.at[index[kind], 1], target)

    def rs1(kind):
        part, got, mid, half, total, col, keep = parts[kind]
        if steps and not heard:
            hear(steps - 1)
            heard.append(True)
        landed(half, rrecv.at[index[kind], 1])
        keep[...] = keep[...] + rooted(half[...])
        total[...] = squared(keep[...])
        for d in range(1, nz):
            peer = lax.rem(z + d, nz)
            send(csend, kind, total.at[peer], col.at[d], crecv.at[index[kind], d], at(peer, y, x))

    def rs2(kind):
        part, got, mid, half, total, col, keep = parts[kind]
        m_ref, s_ref, m_out, s_out = moments[kind]
        for d in range(1, nz):
            landed(col.at[d], crecv.at[index[kind], d])
        g = keep[z]
        for d in range(1, nz):
            g = g + rooted(col[d])
        m = 0.8 * m_ref[...] + 0.2 * g
        s = 0.95 * s_ref[...] + 0.05 * g * g
        m_out[...] = m
        s_out[...] = s
        dfull[kind][me] = (m / (jnp.sqrt(s) + 1e-08)).astype(BF16)
        for d in range(1, nz):
            apush(kind, me, at(lax.rem(z + d, nz), y, x))
        aspread(kind, me)

    def apush(kind, b, target):
        ref = dfull[kind].at[b]
        send(asend, kind, ref, ref, arecv.at[index[kind], b], target)

    def aspread(kind, b):
        for target in (to_y, to_x) if kind == "v" else (to_x, to_y):
            apush(kind, b, target)

    def alanded(kind, b):
        landed(dfull[kind].at[b], arecv.at[index[kind], b])

    def agz(kind, j):
        b = at(planes[j], y, x)
        alanded(kind, b)
        aspread(kind, b)

    def agn(kind, j):
        b = at(planes[j], oy, x) if kind == "v" else at(planes[j], y, ox)
        alanded(kind, b)
        apush(kind, b, to_x if kind == "v" else to_y)

    def whole(kind):
        d = dfull[kind][...]
        if rows % 16:
            return d.astype(F32).reshape(nfs * rows, cols).astype(BF16)
        return d.reshape(nfs * rows, cols)

    def dirs(kind):
        for p in planes:
            alanded(kind, at(p, y, ox) if kind == "v" else at(p, oy, x))
            alanded(kind, at(p, oy, ox))
        if kind == "o":
            turned[...] = whole(kind).T

    def factor_rows(b, r0, n):
        return pl.ds(pl.multiple_of(b * width + r0, 16), n)

    def move_v(b, r0, n):
        return 0.05 * jnp.dot(vfac[factor_rows(b, r0, n), :], whole("v"), preferred_element_type=F32)

    def move_o(b, r0, n):
        return 0.05 * lax.dot_general(
            turned[pl.ds(r0, n), :], ofac[factor_rows(b, 0, width), :],
            (((1,), (1,)), ((), ())), preferred_element_type=F32,
        )

    def put_o(b, r0, n, new):
        if flat:
            o_out[pl.ds(r0, n), pl.ds(pl.multiple_of(b * width, width), width)] = new
        else:
            o_out[b, pl.ds(r0, n), :] = new

    def refresh(kind, b, r0=0, n=None):
        n = size[kind] - r0 if n is None else n
        if kind == "v":
            old = decode(gv[b, pl.ds(r0, n), :])
            v_out[factor_rows(b, r0, n), :] = (old - move_v(b, r0, n)).astype(BF16)
        else:
            old = decode(go[b, pl.ds(r0, n), :])
            put_o(b, r0, n, (old - move_o(b, r0, n)).astype(BF16))

    def own(kind):
        if kind == "v":
            new = vw_in[...] - move_v(me, 0, width)
            v_master[...] = new
            v_out[factor_rows(me, 0, width), :] = new.astype(BF16)
        else:
            new = ow_in[...] - move_o(me, 0, cols)
            o_master[...] = new
            put_o(me, 0, cols, new.astype(BF16))

    waited = {}

    def await_block(what, kind, j, cond=None):
        p = planes[j]
        b, part = {
            "a": (at(p, y, x), None),
            "n": (at(p, oy, x) if kind == "v" else at(p, y, ox), None),
            "m": (at(p, y, ox) if kind == "v" else at(p, oy, x), None),
            "d": (at(p, oy, ox), 1 if j else None),
            "e": (at(p, oy, ox), 0),
        }[what]
        state = waited.get((what, kind, j))
        if state == "all" or (state == "some" and cond is not None):
            return b
        if state == "some":
            arrived(kind, b, part, jnp.logical_not(onward(j)[0]))
        else:
            arrived(kind, b, part, cond)
        waited[what, kind, j] = "all" if cond is None else "some"
        return b

    def zf(kind, j):
        go_on, target = onward(j)
        push(kind, await_block("a", kind, j, go_on), target, cond=go_on)

    def sp(kind, j, link):
        push(kind, await_block("a", kind, j), links[link])

    def nf(kind, j):
        push(kind, await_block("n", kind, j), to_x if kind == "v" else to_y, 1 if j else None)

    def dg(kind):
        b = await_block("d", kind, 0)
        push(kind, b, up, 0, has_up)
        push(kind, b, down, 0, has_down)

    def dz(kind, j):
        go_on, target = onward(j)
        push(kind, await_block("e", kind, j, go_on), target, 0, go_on)

    def update(kind, j, part):
        p = planes[j]
        if part == "d":
            b = await_block("d", kind, j)
            if j:
                await_block("e", kind, j)
            refresh(kind, b)
            return
        if j:
            await_block("a", kind, j)
        await_block("n", kind, j)
        await_block("m", kind, j)
        if j == 0:
            own(kind)

        def step(c, carry):
            cy = jnp.where(c == 2, oy, y)
            cx = jnp.where(c == 1, ox, x)
            refresh(kind, at(p, cy, cx))
            return carry

        lax.fori_loop(0 if j else 1, 3, step, 0)

    ops = {
        "a": own_send, "c": compute, "zf": zf, "sp": sp, "nf": nf, "dg": dg, "dz": dz,
        "ra": ra, "rs1": rs1, "rs2": rs2, "agz": agz, "agn": agn, "dirs": dirs, "up": update,
    }
    for name, *args in schedule(nz):
        ops[name](*args)
    for cond, make in pending:
        when(cond, lambda make=make: make().wait_send())


def publish(count, *refs):
    sems = refs[-1]
    copies = [
        pltpu.make_async_copy(refs[k], refs[count + k], sems.at[k]) for k in range(count)
    ]
    for copy in copies:
        copy.start()
    for copy in copies:
        copy.wait()


def local(
    nfs, ntp,
    inputs, value_cotangent, first_map, second_map, lambdas, head_gain,
    output_cotangent, value_factor, output_factor, value_weight, output_weight,
    value_moment, value_second, output_moment, output_second,
):
    tokens, cols = inputs.shape
    width = value_weight.shape[0]
    rank = value_factor.shape[1]
    rows = value_moment.shape[0]
    nz = nfs // NC
    scale = 1.0 / math.sqrt(tokens * nfs)
    flat = width % 128 == 0
    vmem = pl.BlockSpec(memory_space=pltpu.VMEM)
    hbm = pl.BlockSpec(memory_space=pl.ANY)
    dma = pltpu.SemaphoreType.DMA
    regular = pltpu.SemaphoreType.REGULAR
    moment = jax.ShapeDtypeStruct((rows, cols), F32)
    out_shape = (
        jax.ShapeDtypeStruct((nfs * width, cols), BF16),
        jax.ShapeDtypeStruct((cols, nfs * width) if flat else (nfs, cols, width), BF16),
        jax.ShapeDtypeStruct((width, cols), F32),
        jax.ShapeDtypeStruct((cols, width), F32),
        moment, moment, moment, moment,
    )
    operands = (
        value_weight, output_weight, inputs, value_factor, output_cotangent, output_factor,
        value_cotangent, first_map, second_map,
        value_moment, value_second, output_moment, output_second, lambdas, head_gain.reshape(1, -1),
    )
    spaces = [pltpu.SMEM if operand is lambdas else pltpu.VMEM for operand in operands]
    shapes = [
        ((nfs, width, cols), BF16),
        ((nfs, cols, width), BF16),
        ((tokens, cols), BF16),
        *[((ntp, tokens, rank), F32)] * 2,
        *[((2, 2, nz, rows, cols), BF16)] * 2,
        *[((2, nz, rows, cols), BF16)] * 2,
        *[((nz, rows, cols), BF16)] * 8,
        *[((nz, rows, cols), F32)] * 2,
        *[((nfs, rows, cols), BF16)] * 2,
        ((cols, rank), BF16),
    ]
    sends = 4 + 9 * nz
    outs = pl.pallas_call(
        functools.partial(exchange, nfs, ntp, scale),
        out_shape=tuple(pltpu.VMEM(out.shape, out.dtype) for out in out_shape),
        in_specs=[hbm] * len(operands),
        out_specs=(vmem,) * 8,
        scratch_shapes=[
            *[space(operand.shape, operand.dtype) for space, operand in zip(spaces, operands)],
            *[pltpu.VMEM(shape, dtype) for shape, dtype in shapes],
            dma((2, sends)), dma((2, nfs)), dma((2, nfs)),
            dma((2, ntp)), dma((2, ntp)),
            dma((2, NC)), dma((2, NC)),
            dma((2, nz)), dma((2, nz)),
            dma((2, 5 * nz)), dma((2, nfs)), dma((len(operands),)),
            regular((max(nz - 2, 1),)), regular((max(nz - 2, 1),)),
        ],
        compiler_params=pltpu.CompilerParams(collective_id=0, has_side_effects=True, vmem_limit_bytes=VMEM_LIMIT),
    )(
        *[pltpu.with_memory_space_constraint(operand, pltpu.HBM) for operand in operands],
    )
    outs = pl.pallas_call(
        functools.partial(publish, len(outs)),
        out_shape=out_shape,
        in_specs=[vmem] * len(outs),
        out_specs=(hbm,) * len(outs),
        scratch_shapes=[dma((len(outs),))],
        compiler_params=pltpu.CompilerParams(vmem_limit_bytes=VMEM_LIMIT),
    )(*outs)
    value_copy, output_copy, value_master, output_master, *moments = outs
    if not flat:
        output_copy = output_copy.transpose(1, 0, 2).reshape(cols, nfs * width)
    return (value_master, output_master, *moments, value_copy, output_copy)


VMEM_LIMIT = 40 * 1024 * 1024


def solution(mesh):
    both = P("fs", "tp")
    in_specs = (
        both, both, both, both, P("tp"), P(), both, P(), P(), both, P("tp", "fs"),
        both, both, both, both,
    )
    out_specs = (
        both, P("tp", "fs"), both, both, both, both, P(None, "tp"), P("tp", None),
    )
    body = functools.partial(local, mesh.shape["fs"], mesh.shape["tp"])
    return jax.shard_map(
        body, mesh=mesh, in_specs=in_specs, out_specs=out_specs, check_vma=False
    )
```

```python
import functools
import math

import jax
import jax.numpy as jnp
from jax import lax
from jax.experimental import pallas as pl
from jax.experimental.pallas import tpu as pltpu
from jax.sharding import PartitionSpec as P

F32 = jnp.float32
BF16 = jnp.bfloat16

CODE = 2.0**30
GRAIN = 2.0**40
NX = 2
NY = 2
NC = NX * NY


def encode(w):
    square = (w * CODE) * (w * CODE)
    fourth = square * square
    return jnp.where(w < 0, -fourth, fourth).astype(BF16)


def decode(v):
    v = v.astype(F32)
    size = lax.rsqrt(lax.rsqrt(jnp.maximum(jnp.abs(v), 1e-36))) * (1.0 / CODE)
    return jnp.where(v < 0, -size, size)


def general(nz):
    js = range(1, nz)
    order = [("zf", "v", 1), ("zf", "v", 2), ("ra", "v"), ("rs1", "v"), ("zf", "o", 1), ("zf", "o", 2), ("nf", "v", 0)]
    order += [("ra", "o"), ("rs1", "o"), ("sp", "v", 1, "y"), ("sp", "v", 1, "x"), ("rs2", "v"), ("nf", "o", 0)]
    order += [("sp", "o", 1, "x"), ("sp", "o", 1, "y"), ("rs2", "o")]
    order += [("zf", kind, j) for j in range(3, nz) for kind in ("v", "o")]
    order += [("agz", "v", j) for j in js] + [("agz", "o", j) for j in js]
    order += [("dg", "v"), ("dg", "o")]
    order += [("sp", "v", 2, "y"), ("sp", "v", 2, "x"), ("sp", "o", 2, "x"), ("sp", "o", 2, "y")]
    order += [("agn", kind, j) for kind in ("v", "o") for j in range(nz)]
    order += [("nf", "v", 1), ("nf", "o", 1)]
    for j in range(3, nz):
        order += [("sp", "v", j, "y"), ("sp", "v", j, "x"), ("sp", "o", j, "x"), ("sp", "o", j, "y")]
    order += [("dz", kind, j) for j in (1, 2) for kind in ("v", "o")]
    for kind in ("v", "o"):
        order += [("dirs", kind), ("up", kind, 0, "c"), ("up", kind, 0, "d"), ("nf", kind, 2)]
    order += [("dz", kind, j) for j in range(3, nz) for kind in ("v", "o")]
    for j in js:
        order += [("nf", kind, j) for kind in ("v", "o") if j >= 3]
        order += [("up", kind, j, part) for kind in ("v", "o") for part in ("c", "d")]
    return [
        ("a", "v", "z"), ("a", "o", "z"), ("a", "v", "y"), ("a", "v", "x"),
        ("c", "v"), ("c", "o"), ("a", "o", "x"), ("a", "o", "y"),
    ] + [step for step in order if len(step) < 3 or step[2] < nz]


def squared(g):
    g = g * GRAIN
    return (g * jnp.abs(g)).astype(BF16)


def rooted(v):
    v = v.astype(F32)
    return v * lax.rsqrt(jnp.maximum(jnp.abs(v), 1e-36)) * (1.0 / GRAIN)


STEPS = (
    ("a", "o", "x"), ("a", "v", "y"), ("a", "o", "z"), ("a", "v", "z"), ("c", "o"), ("zf", "o", 1),
    ("nf", "o", 0), ("zf", "o", 2), ("sp", "o", 1, "x"), ("ra", "o"), ("zf", "v", 2), ("zf", "v", 1),
    ("c", "v"), ("sp", "v", 1, "y"), ("sp", "o", 2, "x"), ("ra", "v"), ("nf", "v", 0), ("sp", "v", 2, "y"),
    ("rs1", "o"), ("sp", "v", 2, "x"), ("sp", "o", 2, "y"), ("zf", "v", 3), ("rs1", "v"), ("rs2", "o"),
    ("nf", "v", 2), ("zf", "o", 3), ("agz", "o", 2), ("rs2", "v"), ("sp", "o", 1, "y"), ("agn", "o", 2),
    ("dg", "v"), ("agz", "o", 1), ("agz", "o", 3), ("agn", "v", 0), ("dg", "o"), ("a", "v", "x"),
    ("agz", "v", 1), ("nf", "o", 1), ("agn", "o", 3), ("agz", "v", 3), ("agz", "v", 2), ("dz", "o", 2),
    ("agn", "v", 2), ("agn", "v", 3), ("sp", "o", 3, "y"), ("agn", "v", 1), ("dz", "v", 2),
    ("sp", "o", 3, "x"), ("dz", "o", 1), ("dirs", "v"), ("dz", "v", 1), ("agn", "o", 0), ("sp", "v", 3, "x"),
    ("agn", "o", 1), ("sp", "v", 3, "y"), ("a", "o", "y"), ("dz", "o", 3), ("sp", "v", 1, "x"),
    ("nf", "v", 1), ("dirs", "o"), ("dz", "v", 3), ("up", "v", 0, "c"), ("nf", "o", 2), ("up", "v", 2, "c"),
    ("up", "v", 0, "d"), ("up", "o", 2, "c"), ("up", "o", 3, "c"), ("up", "o", 1, "d"), ("nf", "o", 3),
    ("up", "o", 1, "c"), ("up", "v", 2, "d"), ("nf", "v", 3), ("up", "o", 0, "d"), ("up", "v", 3, "c"),
    ("up", "o", 0, "c"), ("up", "v", 1, "c"), ("up", "v", 1, "d"), ("up", "o", 2, "d"), ("up", "o", 3, "d"),
    ("up", "v", 3, "d"),
)


def schedule(nz):
    return STEPS if nz == 4 else general(nz)


def exchange(
    nfs, ntp, scale,
    vw_hbm, ow_hbm, inp_hbm, vfac_hbm, ocot_hbm, ofac_hbm, vcot_hbm, first_hbm, second_hbm,
    vm_hbm, vs_hbm, om_hbm, os_hbm, lam_hbm, gain_hbm,
    v_out, o_out, v_master, o_master, vm_new, vs_new, om_new, os_new,
    vw_in, ow_in, inp, vfac, ocot, ofac, vcot, first, second, vm, vs, om, os_, lam, gain,
    gv, go, heads, proj_v, proj_o,
    part_v, part_o, got_v, got_o, mid_v, mid_o, half_v, half_o, sum_v, sum_o, col_v, col_o, keep_v, keep_o,
    dfull_v, dfull_o, turned,
    wsend, wrecv, drecv, psend, precv, rsend, rrecv, csend, crecv, asend, arecv, insem, rising, falling,
):
    me = lax.axis_index("fs")
    tp = lax.axis_index("tp")
    tokens, cols = inp.shape
    width = vw_in.shape[0]
    rows = vm.shape[0]
    nz = nfs // NC
    x = lax.rem(me, NX)
    y = lax.rem(lax.div(me, NX), NY)
    z = lax.div(me, NC)
    ox, oy = 1 - x, 1 - y
    cut = {"v": width * 7 // 8 // 16 * 16, "o": cols * 13 // 16 // 16 * 16}
    size = {"v": width, "o": cols}
    index = {"v": 0, "o": 1}
    store = {"v": gv, "o": go}
    flat = len(o_out.shape) == 2

    def when(cond, run):
        if cond is None:
            run()
        else:
            pl.when(cond)(run)

    def at(p, cy, cx):
        return (p * NY + cy) * NX + cx

    below = nz - 1 - z
    pairs = jnp.minimum(z, below)

    def plane(j):
        if j == 0:
            return z
        near = z + (-1 if j % 2 else 1) * ((j + 1) // 2)
        rest = jnp.where(z < below, j, nz - 1 - j)
        return jnp.where(j <= 2 * pairs, near, rest)

    planes = [plane(j) for j in range(nz)]

    def onward(j):
        p = planes[j]
        rising = p < z
        go_on = (rising & (z + 1 < nz)) | (jnp.logical_not(rising) & (z > 0))
        target = at(jnp.where(rising, lax.rem(z + 1, nz), lax.rem(z + nz - 1, nz)), y, x)
        return go_on, target

    to_x, to_y = at(z, y, ox), at(z, oy, x)
    up, down = at(lax.rem(z + 1, nz), y, x), at(lax.rem(z + nz - 1, nz), y, x)
    has_up, has_down = z + 1 < nz, z > 0
    barrier = pltpu.get_barrier_semaphore()
    for target, cond in ((to_x, None), (to_y, None), (up, has_up), (down, has_down)):
        when(cond, lambda target=target: pl.semaphore_signal(barrier, inc=1, device_id={"fs": target}))
    for k in range(1, ntp):
        pl.semaphore_signal(barrier, inc=1, device_id={"tp": lax.rem(tp + k, ntp)})
    loads = {}
    inputs = {
        "vw": (vw_hbm, vw_in), "ow": (ow_hbm, ow_in), "inp": (inp_hbm, inp), "vfac": (vfac_hbm, vfac),
        "ocot": (ocot_hbm, ocot), "ofac": (ofac_hbm, ofac), "vcot": (vcot_hbm, vcot),
        "first": (first_hbm, first), "second": (second_hbm, second),
        "vm": (vm_hbm, vm), "vs": (vs_hbm, vs), "om": (om_hbm, om), "os": (os_hbm, os_),
        "lam": (lam_hbm, lam), "gain": (gain_hbm, gain),
    }
    for k, (name, (src, dst)) in enumerate(inputs.items()):
        loads[name] = pltpu.make_async_copy(src, dst, insem.at[k])
    first_loads = ("vw", "ow", "inp", "vfac")
    for name in first_loads:
        loads[name].start()
    loads["vw"].wait()
    for name in loads:
        if name not in first_loads:
            loads[name].start()
    gv[me] = encode(vw_in[...])
    loads["ow"].wait()
    go[me] = encode(ow_in[...])
    pl.semaphore_wait(barrier, 1 + ntp + jnp.where(has_up, 1, 0) + jnp.where(has_down, 1, 0))

    def tell(k):
        when(has_up, lambda: pl.semaphore_signal(rising.at[k], inc=1, device_id={"fs": up}))
        when(has_down, lambda: pl.semaphore_signal(falling.at[k], inc=1, device_id={"fs": down}))

    def hear(k):
        when(has_down, lambda: pl.semaphore_wait(rising.at[k], 1))
        when(has_up, lambda: pl.semaphore_wait(falling.at[k], 1))

    steps = max(nz - 2, 0)
    if steps:
        tell(0)

    pending = []
    counts = {}

    def send(sems, kind, src, dst, recv, target, cond=None):
        k = counts.get((id(sems), kind), 0)
        counts[(id(sems), kind)] = k + 1

        def make():
            return pltpu.make_async_remote_copy(
                src_ref=src, dst_ref=dst, send_sem=sems.at[index[kind], k],
                recv_sem=recv, device_id={"fs": target},
            )

        when(cond, lambda: make().start())
        pending.append((cond, make))

    def landed(ref, recv, cond=None):
        when(cond, lambda: pltpu.make_async_remote_copy(
            src_ref=ref, dst_ref=ref, send_sem=wsend.at[0, 0], recv_sem=recv,
            device_id={"fs": at(z, y, ox)},
        ).wait_recv())

    def block(kind, b, part=None):
        ref = store[kind].at[b]
        if part is None:
            return ref, wrecv.at[index[kind], b]
        if part == 0:
            return store[kind].at[b, pl.ds(0, cut[kind])], drecv.at[index[kind], lax.div(b, NC)]
        rest = size[kind] - cut[kind]
        return store[kind].at[b, pl.ds(cut[kind], rest)], wrecv.at[index[kind], b]

    def push(kind, b, target, part=None, cond=None):
        ref, recv = block(kind, b, part)
        send(wsend, kind, ref, ref, recv, target, cond)

    def arrived(kind, b, part=None, cond=None):
        ref, recv = block(kind, b, part)
        landed(ref, recv, cond)

    to_x, to_y = at(z, y, ox), at(z, oy, x)
    up, down = at(lax.rem(z + 1, nz), y, x), at(lax.rem(z + nz - 1, nz), y, x)

    links = {"x": to_x, "y": to_y}

    def own_send(kind, link):
        if link == "z":
            push(kind, me, up, cond=has_up)
            push(kind, me, down, cond=has_down)
        else:
            push(kind, me, links[link])

    mine = pl.ds(pl.multiple_of(tp * cols, cols), cols)
    pcopies = {}

    def project(kind, cot, factor, proj):
        proj[0] = jnp.dot(cot[...], factor[mine, :], preferred_element_type=F32)
        pcopies[kind] = []
        for k in range(1, ntp):
            copy = pltpu.make_async_remote_copy(
                src_ref=proj.at[0], dst_ref=proj.at[k],
                send_sem=psend.at[index[kind], k - 1], recv_sem=precv.at[index[kind], k - 1],
                device_id={"tp": lax.rem(tp + k, ntp)},
            )
            copy.start()
            pcopies[kind].append(copy)

    def contract(a, b):
        return lax.dot_general(a, b, (((0,), (0,)), ((), ())), preferred_element_type=F32)

    def reduce_low(kind, proj, right, part, got):
        for copy in pcopies[kind]:
            copy.wait()
        total = proj[0]
        for k in range(1, ntp):
            total = total + proj[k]
        high = total.astype(BF16)
        low = (total - high.astype(F32)).astype(BF16)
        product = (contract(high, right[...]) + contract(low, right[...])) * scale
        for b in range(nfs):
            cy, cx = b // NX % NY, b % NX
            lead, follow = (cx, cy) if kind == "v" else (cy, cx)
            part[lead, follow, b // NC] = squared(product[b * rows:(b + 1) * rows])
        other, target = (ox, to_x) if kind == "v" else (oy, to_y)
        send(rsend, kind, part.at[other], got, rrecv.at[index[kind], 0], target)

    def fetch(*names):
        for name in names:
            loads[name].wait()

    def normalize():
        head_width = gain.shape[1]
        for h in range(cols // head_width):
            span = pl.ds(h * head_width, head_width)
            diff = first[:, span].astype(F32) - lam[h] * second[:, span].astype(F32)
            mean = jnp.mean(diff * diff, axis=-1, keepdims=True)
            heads[:, span] = (diff * lax.rsqrt(mean + 1e-06) * gain[...]).astype(BF16)

    def project_once(kind):
        if kind in pcopies:
            return
        if kind == "v":
            fetch("inp", "vfac")
            project("v", inp, vfac, proj_v)
        else:
            fetch("ocot", "ofac")
            project("o", ocot, ofac, proj_o)

    def compute(kind):
        opening = not pcopies
        project_once(kind)
        project_once("o" if kind == "v" else "v")
        if kind == "v":
            fetch("vcot")
        else:
            fetch("first", "second", "lam", "gain", "vm", "vs", "om", "os")
            normalize()
        if opening:
            for k in range(1, steps):
                hear(k - 1)
                tell(k)
        if kind == "v":
            reduce_low("v", proj_v, vcot, part_v, got_v)
        else:
            reduce_low("o", proj_o, heads, part_o, got_o)

    parts = {
        "v": (part_v, got_v, mid_v, half_v, sum_v, col_v, keep_v),
        "o": (part_o, got_o, mid_o, half_o, sum_o, col_o, keep_o),
    }
    moments = {"v": (vm, vs, vm_new, vs_new), "o": (om, os_, om_new, os_new)}
    dfull = {"v": dfull_v, "o": dfull_o}

    heard = []

    def ra(kind):
        part, got, mid, half, total, col, keep = parts[kind]
        landed(got, rrecv.at[index[kind], 0])
        lead, own, other, target = (x, y, oy, to_y) if kind == "v" else (y, x, ox, to_x)
        keep[...] = rooted(part[lead, own]) + rooted(got[own])
        mid[...] = squared(rooted(part[lead, other]) + rooted(got[other]))
        send(rsend, kind, mid, half, rrecv.at[index[kind], 1], target)

    def rs1(kind):
        part, got, mid, half, total, col, keep = parts[kind]
        if steps and not heard:
            hear(steps - 1)
            heard.append(True)
        landed(half, rrecv.at[index[kind], 1])
        keep[...] = keep[...] + rooted(half[...])
        total[...] = squared(keep[...])
        for d in range(1, nz):
            peer = lax.rem(z + d, nz)
            send(csend, kind, total.at[peer], col.at[d], crecv.at[index[kind], d - 1], at(peer, y, x))

    def rs2(kind):
        part, got, mid, half, total, col, keep = parts[kind]
        m_ref, s_ref, m_out, s_out = moments[kind]
        for d in range(1, nz):
            landed(col.at[d], crecv.at[index[kind], d - 1])
        g = keep[z]
        for d in range(1, nz):
            g = g + rooted(col[d])
        m = 0.8 * m_ref[...] + 0.2 * g
        s = 0.95 * s_ref[...] + 0.05 * g * g
        m_out[...] = m
        s_out[...] = s
        dfull[kind][me] = (m / (jnp.sqrt(s) + 1e-08)).astype(BF16)
        for d in range(1, nz):
            apush(kind, me, at(lax.rem(z + d, nz), y, x))
        aspread(kind, me)

    def apush(kind, b, target):
        ref = dfull[kind].at[b]
        send(asend, kind, ref, ref, arecv.at[index[kind], b], target)

    def aspread(kind, b):
        for target in (to_y, to_x) if kind == "v" else (to_x, to_y):
            apush(kind, b, target)

    def alanded(kind, b):
        landed(dfull[kind].at[b], arecv.at[index[kind], b])

    def agz(kind, j):
        b = at(planes[j], y, x)
        alanded(kind, b)
        aspread(kind, b)

    def agn(kind, j):
        b = at(planes[j], oy, x) if kind == "v" else at(planes[j], y, ox)
        alanded(kind, b)
        apush(kind, b, to_x if kind == "v" else to_y)

    def whole(kind):
        d = dfull[kind][...]
        if rows % 16:
            return d.astype(F32).reshape(nfs * rows, cols).astype(BF16)
        return d.reshape(nfs * rows, cols)

    def dirs(kind):
        for p in planes:
            alanded(kind, at(p, y, ox) if kind == "v" else at(p, oy, x))
            alanded(kind, at(p, oy, ox))
        if kind == "o":
            turned[...] = whole(kind).T

    def factor_rows(b, r0, n):
        return pl.ds(pl.multiple_of(b * width + r0, 16), n)

    def move_v(b, r0, n):
        return 0.05 * jnp.dot(vfac[factor_rows(b, r0, n), :], whole("v"), preferred_element_type=F32)

    def move_o(b, r0, n):
        return 0.05 * lax.dot_general(
            turned[pl.ds(r0, n), :], ofac[factor_rows(b, 0, width), :],
            (((1,), (1,)), ((), ())), preferred_element_type=F32,
        )

    def put_o(b, r0, n, new):
        if flat:
            o_out[pl.ds(r0, n), pl.ds(pl.multiple_of(b * width, width), width)] = new
        else:
            o_out[b, pl.ds(r0, n), :] = new

    def refresh(kind, b, r0=0, n=None):
        n = size[kind] - r0 if n is None else n
        if kind == "v":
            old = decode(gv[b, pl.ds(r0, n), :])
            v_out[factor_rows(b, r0, n), :] = (old - move_v(b, r0, n)).astype(BF16)
        else:
            old = decode(go[b, pl.ds(r0, n), :])
            put_o(b, r0, n, (old - move_o(b, r0, n)).astype(BF16))

    def own(kind):
        if kind == "v":
            new = vw_in[...] - move_v(me, 0, width)
            v_master[...] = new
            v_out[factor_rows(me, 0, width), :] = new.astype(BF16)
        else:
            new = ow_in[...] - move_o(me, 0, cols)
            o_master[...] = new
            put_o(me, 0, cols, new.astype(BF16))

    waited = {}

    def await_block(what, kind, j, cond=None):
        p = planes[j]
        b, part = {
            "a": (at(p, y, x), None),
            "n": (at(p, oy, x) if kind == "v" else at(p, y, ox), None),
            "m": (at(p, y, ox) if kind == "v" else at(p, oy, x), None),
            "d": (at(p, oy, ox), 1 if j else None),
            "e": (at(p, oy, ox), 0),
        }[what]
        state = waited.get((what, kind, j))
        if state == "all" or (state == "some" and cond is not None):
            return b
        if state == "some":
            arrived(kind, b, part, jnp.logical_not(onward(j)[0]))
        else:
            arrived(kind, b, part, cond)
        waited[what, kind, j] = "all" if cond is None else "some"
        return b

    def zf(kind, j):
        go_on, target = onward(j)
        push(kind, await_block("a", kind, j, go_on), target, cond=go_on)

    def sp(kind, j, link):
        push(kind, await_block("a", kind, j), links[link])

    def nf(kind, j):
        push(kind, await_block("n", kind, j), to_x if kind == "v" else to_y, 1 if j else None)

    def dg(kind):
        b = await_block("d", kind, 0)
        push(kind, b, up, 0, has_up)
        push(kind, b, down, 0, has_down)

    def dz(kind, j):
        go_on, target = onward(j)
        push(kind, await_block("e", kind, j, go_on), target, 0, go_on)

    def update(kind, j, part):
        p = planes[j]
        if part == "d":
            b = await_block("d", kind, j)
            if j:
                await_block("e", kind, j)
            refresh(kind, b)
            return
        if j:
            await_block("a", kind, j)
        await_block("n", kind, j)
        await_block("m", kind, j)
        if j == 0:
            own(kind)

        def step(c, carry):
            cy = jnp.where(c == 2, oy, y)
            cx = jnp.where(c == 1, ox, x)
            refresh(kind, at(p, cy, cx))
            return carry

        lax.fori_loop(0 if j else 1, 3, step, 0)

    ops = {
        "a": own_send, "c": compute, "zf": zf, "sp": sp, "nf": nf, "dg": dg, "dz": dz,
        "ra": ra, "rs1": rs1, "rs2": rs2, "agz": agz, "agn": agn, "dirs": dirs, "up": update,
    }
    for name, *args in schedule(nz):
        ops[name](*args)
    for cond, make in pending:
        when(cond, lambda make=make: make().wait_send())


def publish(count, *refs):
    sems = refs[-1]
    copies = [
        pltpu.make_async_copy(refs[k], refs[count + k], sems.at[k]) for k in range(count)
    ]
    for copy in copies:
        copy.start()
    for copy in copies:
        copy.wait()


def local(
    nfs, ntp,
    inputs, value_cotangent, first_map, second_map, lambdas, head_gain,
    output_cotangent, value_factor, output_factor, value_weight, output_weight,
    value_moment, value_second, output_moment, output_second,
):
    tokens, cols = inputs.shape
    width = value_weight.shape[0]
    rank = value_factor.shape[1]
    rows = value_moment.shape[0]
    nz = nfs // NC
    scale = 1.0 / math.sqrt(tokens * nfs)
    flat = width % 128 == 0
    vmem = pl.BlockSpec(memory_space=pltpu.VMEM)
    hbm = pl.BlockSpec(memory_space=pl.ANY)
    dma = pltpu.SemaphoreType.DMA
    regular = pltpu.SemaphoreType.REGULAR
    moment = jax.ShapeDtypeStruct((rows, cols), F32)
    out_shape = (
        jax.ShapeDtypeStruct((nfs * width, cols), BF16),
        jax.ShapeDtypeStruct((cols, nfs * width) if flat else (nfs, cols, width), BF16),
        jax.ShapeDtypeStruct((width, cols), F32),
        jax.ShapeDtypeStruct((cols, width), F32),
        moment, moment, moment, moment,
    )
    operands = (
        value_weight, output_weight, inputs, value_factor, output_cotangent, output_factor,
        value_cotangent, first_map, second_map,
        value_moment, value_second, output_moment, output_second, lambdas, head_gain.reshape(1, -1),
    )
    spaces = [pltpu.SMEM if operand is lambdas else pltpu.VMEM for operand in operands]
    shapes = [
        ((nfs, width, cols), BF16),
        ((nfs, cols, width), BF16),
        ((tokens, cols), BF16),
        *[((ntp, tokens, rank), F32)] * 2,
        *[((2, 2, nz, rows, cols), BF16)] * 2,
        *[((2, nz, rows, cols), BF16)] * 2,
        *[((nz, rows, cols), BF16)] * 8,
        *[((nz, rows, cols), F32)] * 2,
        *[((nfs, rows, cols), BF16)] * 2,
        ((cols, rank), BF16),
    ]
    outs = pl.pallas_call(
        functools.partial(exchange, nfs, ntp, scale),
        out_shape=tuple(pltpu.VMEM(out.shape, out.dtype) for out in out_shape),
        in_specs=[hbm] * len(operands),
        out_specs=(vmem,) * 8,
        scratch_shapes=[
            *[space(operand.shape, operand.dtype) for space, operand in zip(spaces, operands)],
            *[pltpu.VMEM(shape, dtype) for shape, dtype in shapes],
            dma((2, 5 * nz + 2)), dma((2, nfs)), dma((2, nz)),
            dma((2, max(ntp - 1, 1))), dma((2, max(ntp - 1, 1))),
            dma((2, 2)), dma((2, 2)),
            dma((2, max(nz - 1, 1))), dma((2, max(nz - 1, 1))),
            dma((2, 4 * nz - 1)), dma((2, nfs)), dma((len(operands),)),
            regular((max(nz - 2, 1),)), regular((max(nz - 2, 1),)),
        ],
        compiler_params=pltpu.CompilerParams(collective_id=0, has_side_effects=True, vmem_limit_bytes=VMEM_LIMIT),
    )(
        *[pltpu.with_memory_space_constraint(operand, pltpu.HBM) for operand in operands],
    )
    outs = pl.pallas_call(
        functools.partial(publish, len(outs)),
        out_shape=out_shape,
        in_specs=[vmem] * len(outs),
        out_specs=(hbm,) * len(outs),
        scratch_shapes=[dma((len(outs),))],
        compiler_params=pltpu.CompilerParams(vmem_limit_bytes=VMEM_LIMIT),
    )(*outs)
    value_copy, output_copy, value_master, output_master, *moments = outs
    if not flat:
        output_copy = output_copy.transpose(1, 0, 2).reshape(cols, nfs * width)
    return (value_master, output_master, *moments, value_copy, output_copy)


VMEM_LIMIT = 40 * 1024 * 1024


def solution(mesh):
    both = P("fs", "tp")
    in_specs = (
        both, both, both, both, P("tp"), P(), both, P(), P(), both, P("tp", "fs"),
        both, both, both, both,
    )
    out_specs = (
        both, P("tp", "fs"), both, both, both, both, P(None, "tp"), P("tp", None),
    )
    body = functools.partial(local, mesh.shape["fs"], mesh.shape["tp"])
    return jax.shard_map(
        body, mesh=mesh, in_specs=in_specs, out_specs=out_specs, check_vma=False
    )
```
